128 devices in a mesh: kv: 32 (over z, y, core), tp: 4 (over x).
Axes of the slice: x: 4, y: 4, z: 4, core: 2. Of those that a mesh axis runs over, the one named last changes fastest.
Arguments:
- tokens: bfloat16 [20480, 4096], P('kv'), may hold values from -48 to 48
- query_weight: bfloat16 [4096, 2048], P(None, 'tp'), may hold values from -0.09375 to 0.09375
- key_weight: bfloat16 [4096, 512], P(None, 'tp'), may hold values from -0.09375 to 0.09375
- value_weight: bfloat16 [4096, 512], P(None, 'tp'), may hold values from -0.09375 to 0.09375
- gate_weight: bfloat16 [4096, 64], replicated, may hold values from -0.09375 to 0.09375
- summary_pos: bfloat16 [32, 64], replicated, may hold values from -6 to 6
- key_mixing: bfloat16 [32, 8], replicated, may hold values from -1 to 1
- value_mixing: bfloat16 [32, 8], replicated, may hold values from -1 to 1
- out_weight: bfloat16 [2048, 4096], P('tp'), may hold values from -0.125 to 0.125
- chosen: int32 [320, 8, 16], P('kv', 'tp'), may hold values from 0 to 319, as said below
Outputs:
- mixed: bfloat16 [20480, 4096], P(('kv', 'tp'))
The draws below stay inside these ranges and needn't reach their ends.
Inputs may be any that keep to these rules, and one draw needn't show every extreme that they name: `chosen`: entry [b, g, 0] is b itself; every entry is at most b. For the query blocks of one index of kv, one key head and any OTHER index of kv, at most 2 distinct blocks of that index's 64-position blocks are named, and exactly 2 of the index just before. Entries may repeat.
All inputs are finite; a program needn't handle non-finite values.
Results may differ from the reference program's by a relative error of at most 0.013.
The reference program's roundings to bfloat16 on the way count: a program that leaves them out, or rounds other values in their place, can miss the bound.
Values may be sent and summed in bfloat16 or wider, within the bound.
A program may use at most 192 MiB of HBM per device.

```python
import jax
import jax.numpy as jnp
from jax import lax

D = 4096
HEADS = 32
KV_HEADS = 8
HD = 64
CMP = 32
SB = 64
N_SEL = 16
CAP = 2
TOK_DEV = 640
TOKENS = 20480
N_TP = 4


def draw_tokens(key, part):
    base = jax.random.normal(key, (TOKENS, D), jnp.float32)
    return jnp.clip(base, -6.0, 6.0).astype(jnp.bfloat16)


def draw_chosen(key, part):
    per_device = TOK_DEV // SB
    block_total = TOKENS // SB
    device_total = block_total // per_device
    grid_shape = (block_total, KV_HEADS, N_SEL)
    column_shape = (block_total, KV_HEADS, 1)
    streams = jax.random.split(key, 8)
    query_block = jnp.arange(block_total, dtype=jnp.int32)[:, None, None]
    device_of = query_block // per_device
    head_ids = jnp.arange(KV_HEADS, dtype=jnp.int32)[None, :, None]
    first_pick = jax.random.randint(streams[0], (device_total, KV_HEADS, device_total), 0, per_device)
    pick_step = jax.random.randint(streams[1], (device_total, KV_HEADS, device_total), 1, per_device)
    popular = jax.random.randint(streams[2], (4,), 0, device_total)
    use_popular = jax.random.randint(streams[3], grid_shape, 0, 2)
    popular_pick = popular[jax.random.randint(streams[4], grid_shape, 0, 4)]
    drawn_pick = jax.random.randint(streams[5], grid_shape, 0, device_of + 1)
    source = jnp.where((use_popular == 1) & (popular_pick <= device_of), popular_pick, drawn_pick)
    which = jax.random.randint(streams[6], grid_shape, 0, CAP)
    candidate = (first_pick[device_of, head_ids, source] + which * pick_step[device_of, head_ids, source]) % per_device
    at_home = jax.random.randint(streams[7], grid_shape, device_of * per_device, query_block + 1)
    picks = jnp.where(source == device_of, at_home, source * per_device + candidate)
    before = jnp.maximum(device_of - 1, 0)
    half_away = jnp.maximum(device_of - device_total // 2, 0)
    first_before = first_pick[device_of, head_ids, before]
    own_block = jnp.broadcast_to(query_block, column_shape)
    slot_one = jnp.where(device_of >= 1, before * per_device + first_before, own_block)
    slot_two = jnp.where(device_of >= device_total // 2, half_away * per_device + first_pick[device_of, head_ids, half_away], own_block)
    slot_three = jnp.where(device_of >= 1, before * per_device + (first_before + pick_step[device_of, head_ids, before]) % per_device, own_block)
    return jnp.concatenate([own_block, jnp.broadcast_to(slot_one, column_shape), jnp.broadcast_to(slot_two, column_shape), jnp.broadcast_to(slot_three, column_shape), picks[:, :, 4:]], axis=2).astype(jnp.int32)


def shard_levels(stream_key, shape, pieces, smallest, high):
    def one(position, shards_of):
        draws = jax.random.uniform(jax.random.fold_in(jax.random.fold_in(stream_key, 6), position), (shards_of,), jnp.float32, smallest / len(pieces), high / len(pieces))
        return jnp.repeat(jnp.exp(draws), shape[position] // shards_of).reshape((-1,) + (1,) * (len(shape) - position - 1))

    gain = one(*pieces[0])
    for cut in pieces[1:]:
        gain = gain * one(*cut)
    return gain


def bell_draw(rng, extent, spread, most, cuts=(), kind=jnp.bfloat16):
    result = jax.random.normal(rng, extent, jnp.float32) * spread
    if len(cuts) > 0:
        result = shard_levels(rng, extent, cuts, -0.22, 0.18) * result
    return jnp.clip(result, min=-most, max=most).astype(kind)


def setup_inputs(seed: int = 0) -> dict:
    arg_keys = jax.random.split(jax.random.key(seed), 11)
    return {
        "tokens": draw_tokens(jax.random.fold_in(arg_keys[10], 71), 0),
        "query_weight": bell_draw(arg_keys[1], (D, HEADS * HD), D ** -0.5, 0.09375, ((1, 4),)),
        "key_weight": bell_draw(arg_keys[2], (D, KV_HEADS * HD), D ** -0.5, 0.09375, ((1, 4),)),
        "value_weight": bell_draw(arg_keys[3], (D, KV_HEADS * HD), D ** -0.5, 0.09375, ((1, 4),)),
        "gate_weight": bell_draw(arg_keys[4], (D, 2 * HEADS), D ** -0.5, 0.09375),
        "summary_pos": bell_draw(arg_keys[5], (CMP, HD), 1.0, 6.0),
        "key_mixing": bell_draw(arg_keys[6], (CMP, KV_HEADS), CMP ** -0.5, 1.0),
        "value_mixing": bell_draw(arg_keys[7], (CMP, KV_HEADS), CMP ** -0.5, 1.0),
        "out_weight": bell_draw(arg_keys[8], (HEADS * HD, D), (HEADS * HD) ** -0.5, 0.125, ((0, 4),)),
        "chosen": draw_chosen(jax.random.fold_in(arg_keys[10], 71), 0),
    }


floor_score = -1e30


def masked_weights(scores, visible):
    probs = jax.nn.softmax(jnp.where(visible, scores, floor_score), axis=-1)
    return jnp.where(jnp.any(visible, axis=-1, keepdims=True), probs, 0.0)


def first_named(picked_ids):
    slot_count = picked_ids.shape[-1]
    repeated = picked_ids[..., :, None] == picked_ids[..., None, :]
    earlier = jnp.arange(slot_count)[None, :] < jnp.arange(slot_count)[:, None]
    return jnp.logical_not(jnp.any(repeated & earlier, axis=-1))


def summarize(source, offsets, mixing):
    span_count = source.shape[0] // CMP
    windows = source.astype(jnp.float32).reshape(span_count, CMP, source.shape[1], HD)
    windows = windows + offsets.astype(jnp.float32)[None, :, None, :]
    return jnp.einsum('njgd,jg->ngd', windows, mixing.astype(jnp.float32),
                      precision=lax.Precision.HIGHEST).astype(jnp.bfloat16)


def reference(tokens, query_weight, key_weight, value_weight, gate_weight, summary_pos, key_mixing,
              value_mixing, out_weight, chosen):
    length = tokens.shape[0]
    group_size = HEADS // KV_HEADS
    score_scale = HD ** -0.5
    queries = jnp.dot(tokens, query_weight, preferred_element_type=jnp.float32).astype(jnp.bfloat16)
    key_rows = jnp.dot(tokens, key_weight, preferred_element_type=jnp.float32).astype(jnp.bfloat16)
    key_rows = key_rows.reshape(length, KV_HEADS, HD)
    value_rows = jnp.dot(tokens, value_weight, preferred_element_type=jnp.float32).astype(jnp.bfloat16)
    value_rows = value_rows.reshape(length, KV_HEADS, HD)
    gate_vals = jax.nn.sigmoid(jnp.dot(tokens, gate_weight, preferred_element_type=jnp.float32))
    gate_vals = gate_vals.reshape(length // SB, SB, KV_HEADS, group_size, 2)
    key_summary = summarize(key_rows, summary_pos, key_mixing).astype(jnp.float32)
    value_summary = summarize(value_rows, summary_pos, value_mixing).astype(jnp.float32)
    span_ends = jnp.arange(length // CMP, dtype=jnp.int32) * CMP + (CMP - 1)
    block_table = jnp.concatenate([key_rows, value_rows], axis=-1).reshape(length // SB, SB, KV_HEADS, 2 * HD)
    head_ids = jnp.arange(KV_HEADS, dtype=jnp.int32)[:, None]
    unique_all = first_named(chosen)

    def one_block(inputs):
        query_blk, gate_blk, picked_ids, unique, offset = inputs
        query_pos = offset + jnp.arange(SB, dtype=jnp.int32)
        query_f = query_blk.astype(jnp.float32).reshape(SB, KV_HEADS, group_size, HD)
        summary_scores = jnp.einsum('qgrd,ngd->grqn', query_f, key_summary) * score_scale
        summary_probs = masked_weights(summary_scores, (span_ends[None, :] <= query_pos[:, None])[None, None])
        summary_probs = lax.optimization_barrier(summary_probs.astype(jnp.bfloat16)).astype(jnp.float32)
        summary_out = jnp.einsum('grqn,ngd->qgrd', summary_probs, value_summary)
        picked = block_table[picked_ids, :, head_ids, :]
        picked = picked.reshape(KV_HEADS, N_SEL * SB, 2 * HD).astype(jnp.float32)
        key_pos = (picked_ids[:, :, None] * SB + jnp.arange(SB, dtype=jnp.int32)).reshape(KV_HEADS, N_SEL * SB)
        counted = jnp.broadcast_to(unique[:, :, None], (KV_HEADS, N_SEL, SB)).reshape(KV_HEADS, N_SEL * SB)
        visible = counted[:, None, :] & (key_pos[:, None, :] <= query_pos[None, :, None])
        chosen_scores = jnp.einsum('qgrd,gmd->grqm', query_f, picked[..., :HD]) * score_scale
        chosen_probs = masked_weights(chosen_scores, visible[:, None])
        chosen_probs = lax.optimization_barrier(chosen_probs.astype(jnp.bfloat16)).astype(jnp.float32)
        chosen_out = jnp.einsum('grqm,gmd->qgrd', chosen_probs, picked[..., HD:])
        blended = gate_blk[..., 0:1] * summary_out + gate_blk[..., 1:2] * chosen_out
        return blended.reshape(SB, HEADS * HD).astype(jnp.bfloat16)

    offsets = jnp.arange(length // SB, dtype=jnp.int32) * SB
    attention = lax.map(one_block, (queries.reshape(length // SB, SB, HEADS * HD), gate_vals, chosen,
                                    unique_all, offsets)).reshape(length, HEADS * HD)
    width = HEADS * HD // N_TP
    summed = jnp.zeros((length, D), jnp.float32)
    for head_part in range(N_TP):
        partial_value = jnp.dot(attention[:, head_part * width:(head_part + 1) * width],
                          out_weight[head_part * width:(head_part + 1) * width],
                          preferred_element_type=jnp.float32).astype(jnp.bfloat16)
        summed = summed + lax.optimization_barrier(partial_value).astype(jnp.float32)
    return summed.astype(jnp.bfloat16)
```

```python
import jax
import jax.numpy as jnp
from jax import lax
from jax.experimental import pallas as pl
from jax.experimental.pallas import tpu as pltpu
from jax.sharding import Mesh
from jax.sharding import PartitionSpec as P

HD = 64
CMP = 32
SB = 64
N_SEL = 16
N_KV = 32
N_TP = 4
ROWS = 640
BLOCKS = 10
GROUPS = 2
GROUP = 4
SPANS = 20
WIDTH = 512
D = 4096
CHUNK = 1024
KV = ("kv_0", "kv_1", "kv_2")
KV_TP = ("kv_0", "kv_1", "kv_2", "tp")
MESH = pl.DeviceIdType.MESH
BF16 = jnp.bfloat16
F32 = jnp.float32
LOW = -1e30


def nt_dot(a, b):
    return lax.dot_general(a, b, (((1,), (1,)), ((), ())), preferred_element_type=F32)


def nn_dot(a, b):
    return jnp.dot(a, b, preferred_element_type=F32)


def body(
    tok_hbm,
    wq_hbm,
    wk_hbm,
    wv_hbm,
    wg_hbm,
    pos_ref,
    kmix_ref,
    vmix_ref,
    need_ref,
    idx_ref,
    bias_ref,
    out_ref,
    tok,
    wq,
    wkv,
    wg,
    acc,
    gates,
    qp,
    sums,
    asked,
    asked_s,
    table,
    stage,
    mine,
    comp,
    load_sem,
    asked_sem,
    need_send,
    need_recv,
    sum_send,
    sum_recv,
    blk_send,
    blk_recv,
):
    kz, ky, kc, x = (lax.axis_index(name) for name in KV_TP)
    me = kz * 8 + ky * 2 + kc

    def at(d):
        return (d // 8, lax.rem(d // 2, 4), lax.rem(d, 2), x)

    barrier = pltpu.get_barrier_semaphore()

    def greet(d, carry):
        @pl.when(d != me)
        def _():
            pl.semaphore_signal(barrier, inc=1, device_id=at(d), device_id_type=MESH)

        return carry

    lax.fori_loop(0, N_KV, greet, 0)

    loads = []

    def load(src, dst):
        loads.append(pltpu.make_async_copy(src, dst, load_sem.at[len(loads)]))
        loads[-1].start()
        return loads[-1]

    steps = D // CHUNK
    kv_loads = []
    for k in range(steps):
        rows = pl.ds(k * CHUNK, CHUNK)
        kv_loads.append(
            (
                load(wk_hbm.at[rows], wkv.at[rows, pl.ds(0, 128)]),
                load(wv_hbm.at[rows], wkv.at[rows, pl.ds(128, 128)]),
                load(tok_hbm.at[:, rows], tok.at[:, rows]),
            )
        )
    wg_load = load(wg_hbm, wg)
    wq_load = load(wq_hbm, wq)

    def clear(d, carry):
        sums[d] = jnp.zeros(sums.shape[1:], BF16)
        return carry

    lax.fori_loop(me + 1, N_KV, clear, 0)
    pl.semaphore_wait(barrier, N_KV - 1)

    def need_copy(d, sender):
        return pltpu.make_async_remote_copy(
            src_ref=need_ref.at[d],
            dst_ref=asked.at[sender],
            send_sem=need_send.at[d],
            recv_sem=need_recv.at[sender],
            device_id=at(d),
            device_id_type=MESH,
        )

    def send_need(d, carry):
        need_copy(d, me).start()
        return carry

    lax.fori_loop(0, me, send_need, 0)

    for k in range(steps):
        for copy in kv_loads[k]:
            copy.wait()
        part = nn_dot(tok[:, k * CHUNK : (k + 1) * CHUNK], wkv[k * CHUNK : (k + 1) * CHUNK])
        acc[...] = part if k == 0 else acc[...] + part
    low = lax.broadcasted_iota(jnp.int32, (ROWS, 128), 1) < HD
    keys = acc[:, :128].astype(BF16).astype(F32)
    values = acc[:, 128:].astype(BF16).astype(F32)
    pairs = (
        jnp.where(low, keys, pltpu.roll(values, HD, 1)),
        jnp.where(low, pltpu.roll(keys, HD, 1), values),
    )
    offsets = pos_ref[...].astype(F32)
    offsets = jnp.concatenate([offsets, offsets], axis=1)
    lane_low = lax.broadcasted_iota(jnp.int32, (CMP, 128), 1) < HD
    lane_head = lax.broadcasted_iota(jnp.int32, (CMP, 8), 1)
    for g in range(GROUPS):
        pair = pairs[g]
        blocks = pair.astype(BF16).reshape(BLOCKS, SB, 128)
        mine[g] = blocks
        table[4 * N_KV + g * BLOCKS : 4 * N_KV + (g + 1) * BLOCKS] = blocks
        own = lane_head == x * GROUPS + g
        kmix = jnp.sum(jnp.where(own, kmix_ref[...].astype(F32), 0.0), axis=1, keepdims=True)
        vmix = jnp.sum(jnp.where(own, vmix_ref[...].astype(F32), 0.0), axis=1, keepdims=True)
        mixing = jnp.where(lane_low, kmix, vmix)
        spans = jnp.sum((pair.reshape(SPANS, CMP, 128) + offsets[None]) * mixing[None], axis=1)
        sums[me, 0, g] = spans[:16].astype(BF16)
        sums[me, 1, g] = jnp.concatenate([spans[16:], jnp.zeros((12, 128), F32)], axis=0).astype(
            BF16
        )

    def sum_copy(d, sender):
        return pltpu.make_async_remote_copy(
            src_ref=sums.at[sender],
            dst_ref=sums.at[sender],
            send_sem=sum_send.at[d],
            recv_sem=sum_recv.at[sender],
            device_id=at(d),
            device_id_type=MESH,
        )

    def send_sum(d, carry):
        sum_copy(d, me).start()
        return carry

    lax.fori_loop(me + 1, N_KV, send_sum, 0)

    def take_need(d, carry):
        need_copy(me, d).wait_recv()
        copy = pltpu.make_async_copy(asked.at[d], asked_s.at[d], asked_sem.at[d])
        copy.start()
        return carry

    lax.fori_loop(me + 1, N_KV, take_need, 0)

    def blk_copy(d, sender):
        return pltpu.make_async_remote_copy(
            src_ref=stage.at[d],
            dst_ref=table.at[pl.ds(sender * 4, 4)],
            send_sem=blk_send.at[d],
            recv_sem=blk_recv.at[sender],
            device_id=at(d),
            device_id_type=MESH,
        )

    def send_blk(d, carry):
        pltpu.make_async_copy(asked.at[d], asked_s.at[d], asked_sem.at[d]).wait()
        for slot in range(4):
            block = asked_s[d, 0, slot]
            stage[d, slot] = mine[slot // 2, block]
        blk_copy(d, me).start()
        return carry

    lax.fori_loop(me + 1, N_KV, send_blk, 0)

    wq_load.wait()
    for g in range(GROUPS):
        cols = slice(256 * g, 256 * (g + 1))
        for k in range(steps):
            ks = slice(k * CHUNK, (k + 1) * CHUNK)
            part = nn_dot(tok[:, ks], wq[ks, cols])
            acc[...] = part if k == 0 else acc[...] + part
        for r in range(GROUP):
            tile = acc[:, 128 * (r // 2) : 128 * (r // 2) + 128]
            if r % 2:
                tile = pltpu.roll(tile, HD, 1)
            tile = jnp.where(low, tile, 0.0).astype(BF16) * BF16(HD**-0.5)
            qp[:, g, r] = tile.reshape(BLOCKS, SB, 128)
    wg_load.wait()
    pick = lax.broadcasted_iota(jnp.int32, (64, 128), 0) == (
        lax.broadcasted_iota(jnp.int32, (64, 128), 1) + x * 16
    )
    own_gates = nn_dot(wg[...], jnp.where(pick, 1.0, 0.0).astype(BF16)).astype(BF16)
    gates[...] = jax.nn.sigmoid(nn_dot(tok[...], own_gates)).reshape(BLOCKS, SB, 128)

    def take_sum(s, carry):
        sum_copy(me, s).wait_recv()
        return carry

    lax.fori_loop(0, me, take_sum, 0)
    lane_a = lax.broadcasted_iota(jnp.int32, (GROUP * SB, 512), 1)
    end_a = ((lane_a // 16) * SPANS + lax.rem(lane_a, 16)) * CMP + CMP - 1
    lane_b = lax.broadcasted_iota(jnp.int32, (GROUP * SB, 128), 1)
    end_b = ((lane_b // 4) * SPANS + 16 + lax.rem(lane_b, 4)) * CMP + CMP - 1
    row_a = lax.rem(lax.broadcasted_iota(jnp.int32, (GROUP * SB, 512), 0), SB)
    row_b = lax.rem(lax.broadcasted_iota(jnp.int32, (GROUP * SB, 128), 0), SB)
    row_c = lax.rem(lax.broadcasted_iota(jnp.int32, (GROUP * SB, 1), 0), SB)
    gap_a = end_a - row_a
    gap_b = end_b - row_b

    def gate_cols(b, g, branch):
        cols = [
            gates[b][:, 2 * (GROUP * g + r) + branch : 2 * (GROUP * g + r) + branch + 1]
            for r in range(GROUP)
        ]
        return jnp.concatenate(cols, axis=0)

    for g in range(GROUPS):
        span_a = sums[:, 0, g].reshape(N_KV * 16, 128)
        span_b = jnp.concatenate([sums[s, 1, g].astype(F32)[:4] for s in range(N_KV)], axis=0)
        span_b = span_b.astype(BF16)

        def compressed(b, carry):
            q = qp[b, g].reshape(GROUP * SB, 128)
            start = me * ROWS + b * SB
            score_a = jnp.where(gap_a <= start, nt_dot(q, span_a), LOW)
            score_b = jnp.where(gap_b <= start, nt_dot(q, span_b), LOW)
            most = jnp.maximum(
                jnp.max(score_a, axis=1, keepdims=True), jnp.max(score_b, axis=1, keepdims=True)
            )
            prob_a = jnp.exp(score_a - most)
            prob_b = jnp.exp(score_b - most)
            total = jnp.sum(prob_a, axis=1, keepdims=True) + jnp.sum(prob_b, axis=1, keepdims=True)
            mixed = nn_dot(prob_a.astype(BF16), span_a) + nn_dot(prob_b.astype(BF16), span_b)
            sees = row_c + start >= CMP - 1
            factor = jnp.where(sees, gate_cols(b, g, 0) / total, 0.0)
            comp[b, g] = mixed * factor
            return carry

        lax.fori_loop(0, BLOCKS, compressed, 0)

    def take_blk(s, carry):
        blk_copy(me, s).wait_recv()
        return carry

    lax.fori_loop(0, me, take_blk, 0)
    lane_first = lax.broadcasted_iota(jnp.int32, (GROUP * SB, 128), 1)
    causal = jnp.logical_or(lane_first >= SB, lane_first <= row_b)
    low_half = lax.broadcasted_iota(jnp.int32, (SB, 128), 1) < HD

    def chosen_block(b, carry):
        for g in range(GROUPS):
            q = qp[b, g].reshape(GROUP * SB, 128)
            base = (b * GROUPS + g) * N_SEL
            picked = jnp.concatenate([table[idx_ref[base + s]] for s in range(N_SEL)], axis=0)
            score = nt_dot(q, picked) + bias_ref[b * GROUPS + g]
            head = jnp.where(causal, score[:, :128], LOW)
            score = jnp.concatenate([head, score[:, 128:]], axis=1)
            most = jnp.max(score, axis=1, keepdims=True)
            prob = jnp.exp(score - most)
            total = jnp.sum(prob, axis=1, keepdims=True)
            mixed = nn_dot(prob.astype(BF16), picked)
            both = comp[b, g] + mixed * (gate_cols(b, g, 1) / total)
            for half in range(2):
                even = both[(2 * half) * SB : (2 * half + 1) * SB]
                odd = both[(2 * half + 1) * SB : (2 * half + 2) * SB]
                tile = jnp.where(low_half, pltpu.roll(even, HD, 1), odd).astype(BF16)
                lanes = slice(256 * g + 128 * half, 256 * g + 128 * half + 128)
                out_ref[pl.ds(pl.multiple_of(b * SB, SB), SB), lanes] = tile
        return carry

    lax.fori_loop(0, BLOCKS, chosen_block, 0)

    def sent_need(d, carry):
        need_copy(d, me).wait_send()
        return carry

    lax.fori_loop(0, me, sent_need, 0)

    def sent_rest(d, carry):
        sum_copy(d, me).wait_send()
        blk_copy(d, me).wait_send()
        return carry

    lax.fori_loop(me + 1, N_KV, sent_rest, 0)


def plan(chosen, me):
    named = chosen.transpose(1, 0, 2).reshape(GROUPS, BLOCKS * N_SEL)
    source = named // BLOCKS
    place = named - source * BLOCKS
    hit = source[:, None, :] == jnp.arange(N_KV, dtype=jnp.int32)[None, :, None]
    first = jnp.min(jnp.where(hit, place[:, None, :], BLOCKS), axis=2)
    last = jnp.max(jnp.where(hit, place[:, None, :], 0), axis=2)
    first_there = jnp.sum(jnp.where(hit, first[:, :, None], 0), axis=1)
    first = jnp.where(first == BLOCKS, 0, first)
    group = jnp.arange(GROUPS, dtype=jnp.int32)[:, None]
    far = (source * GROUPS + group) * 2 + (place != first_there).astype(jnp.int32)
    near = 4 * N_KV + group * BLOCKS + place
    index = jnp.where(source == me, near, far)
    index = index.reshape(GROUPS, BLOCKS, N_SEL).transpose(1, 0, 2).reshape(-1)
    need = jnp.stack([first, last], axis=-1).transpose(1, 0, 2).reshape(N_KV, 1, 2 * GROUPS)
    need = jnp.pad(need, ((0, 0), (0, 0), (0, 128 - 2 * GROUPS)))
    same = chosen[..., :, None] == chosen[..., None, :]
    slot = jnp.arange(N_SEL, dtype=jnp.int32)
    repeated = jnp.any(same & (slot[None, :] < slot[:, None]), axis=-1)
    bias = jnp.where(repeated, LOW, 0.0).astype(F32)
    bias = jnp.repeat(bias, SB, axis=-1).reshape(BLOCKS * GROUPS, 1, N_SEL * SB)
    return need, index, bias


def local(
    tokens,
    query_weight,
    key_weight,
    value_weight,
    gate_weight,
    summary_pos,
    key_mixing,
    value_mixing,
    out_weight,
    chosen,
):
    need, index, bias = plan(chosen, lax.axis_index(KV))
    any_space = pl.BlockSpec(memory_space=pl.ANY)
    vmem = pl.BlockSpec(memory_space=pltpu.VMEM)
    smem = pl.BlockSpec(memory_space=pltpu.SMEM)
    dma = pltpu.SemaphoreType.DMA
    attention = pl.pallas_call(
        body,
        out_shape=jax.ShapeDtypeStruct((ROWS, WIDTH), BF16),
        in_specs=[any_space] * 5 + [vmem] * 4 + [smem, vmem],
        out_specs=vmem,
        scratch_shapes=[
            pltpu.VMEM((ROWS, D), BF16),
            pltpu.VMEM((D, WIDTH), BF16),
            pltpu.VMEM((D, 256), BF16),
            pltpu.VMEM((D, 64), BF16),
            pltpu.VMEM((ROWS, 256), F32),
            pltpu.VMEM((BLOCKS, SB, 128), F32),
            pltpu.VMEM((BLOCKS, GROUPS, GROUP, SB, 128), BF16),
            pltpu.VMEM((N_KV, 2, GROUPS, 16, 128), BF16),
            pltpu.VMEM((N_KV, 1, 128), jnp.int32),
            pltpu.SMEM((N_KV, 1, 128), jnp.int32),
            pltpu.VMEM((4 * N_KV + GROUPS * BLOCKS, SB, 128), BF16),
            pltpu.VMEM((N_KV, 4, SB, 128), BF16),
            pltpu.VMEM((GROUPS, BLOCKS, SB, 128), BF16),
            pltpu.VMEM((BLOCKS, GROUPS, GROUP * SB, 128), F32),
            dma((16,)),
            dma((N_KV,)),
            dma((N_KV,)),
            dma((N_KV,)),
            dma((N_KV,)),
            dma((N_KV,)),
            dma((N_KV,)),
            dma((N_KV,)),
        ],
        compiler_params=pltpu.CompilerParams(
            collective_id=0, has_side_effects=True, vmem_limit_bytes=63 * 1024 * 1024
        ),
    )(
        tokens,
        query_weight,
        key_weight,
        value_weight,
        gate_weight,
        summary_pos,
        key_mixing,
        value_mixing,
        need,
        index,
        bias,
    )
    return lax.psum_scatter(
        jnp.dot(attention, out_weight, preferred_element_type=F32).astype(BF16),
        "tp",
        scatter_dimension=0,
        tiled=True,
    )


def solution(mesh):
    torus = Mesh(mesh.devices.reshape(4, 4, 2, mesh.shape["tp"]), ("kv_0", "kv_1", "kv_2", "tp"))
    in_specs = (
        P(KV, None),
        P(None, "tp"),
        P(None, "tp"),
        P(None, "tp"),
        P(),
        P(),
        P(),
        P(),
        P("tp", None),
        P(KV, "tp", None),
    )
    out_specs = P(KV_TP, None)
    return jax.shard_map(local, mesh=torus, in_specs=in_specs, out_specs=out_specs, check_vma=False)
```

```python
import jax
import jax.numpy as jnp
from jax import lax
from jax.experimental import pallas as pl
from jax.experimental.pallas import tpu as pltpu
from jax.sharding import Mesh
from jax.sharding import PartitionSpec as P

HD = 64
CMP = 32
SB = 64
N_SEL = 16
N_KV = 32
N_TP = 4
ROWS = 640
BLOCKS = 10
GROUPS = 2
GROUP = 4
SPANS = 20
WIDTH = 512
OUT_ROWS = 160
D = 4096
CHUNK = 1024
KV = ("kv_0", "kv_1", "kv_2")
KV_TP = ("kv_0", "kv_1", "kv_2", "tp")
MESH = pl.DeviceIdType.MESH
BF16 = jnp.bfloat16
F32 = jnp.float32
LOW = -1e30


def nt_dot(a, b):
    return lax.dot_general(a, b, (((1,), (1,)), ((), ())), preferred_element_type=F32)


def nn_dot(a, b):
    return jnp.dot(a, b, preferred_element_type=F32)


def make_plan(chosen_ref, need_ref, bias_ref):
    lane = lax.broadcasted_iota(jnp.int32, (BLOCKS, N_SEL), 1)
    spread = lax.broadcasted_iota(jnp.int32, (N_SEL, N_SEL * SB), 1) // SB
    spread = spread == lax.broadcasted_iota(jnp.int32, (N_SEL, N_SEL * SB), 0)
    spread = jnp.where(spread, 1.0, 0.0).astype(BF16)
    need_lane = lax.broadcasted_iota(jnp.int32, (1, 128), 1)
    named = [chosen_ref[:, g, :] for g in range(GROUPS)]
    for g in range(GROUPS):
        repeated = jnp.zeros((BLOCKS, N_SEL), F32)
        for t in range(N_SEL - 1):
            same = jnp.logical_and(named[g] == named[g][:, t : t + 1], lane > t)
            repeated = jnp.where(same, 1.0, repeated)
        bias = nn_dot(repeated.astype(BF16), spread) * LOW
        for b in range(BLOCKS):
            bias_ref[g, b] = bias[b : b + 1]
    places = [n - (n // BLOCKS) * BLOCKS for n in named]
    sources = [n // BLOCKS for n in named]

    def ends(axis_min, value):
        for axis in (0, 1):
            value = axis_min(value, axis=axis, keepdims=True)
        return value

    for s in range(N_KV):
        row = jnp.zeros((1, 128), jnp.int32)
        for g in range(GROUPS):
            hit = sources[g] == s
            first = ends(jnp.min, jnp.where(hit, places[g], BLOCKS - 1))
            last = ends(jnp.max, jnp.where(hit, places[g], 0))
            row = jnp.where(need_lane == 2 * g, first, row)
            row = jnp.where(need_lane == 2 * g + 1, last, row)
        need_ref[s] = row


def body(
    tok_hbm,
    wq_hbm,
    wk_hbm,
    wv_hbm,
    wg_hbm,
    pos_ref,
    kmix_ref,
    vmix_ref,
    wo_hbm,
    chosen_ref,
    chosen_s,
    out_ref,
    tok,
    wq,
    wkv,
    wg,
    acc,
    gates,
    qp,
    sums,
    asked,
    asked_s,
    table,
    stage,
    mine,
    comp,
    need_ref,
    need_s,
    bias_ref,
    wall,
    att,
    got,
    total_ref,
    load_sem,
    asked_sem,
    w_send,
    w_recv,
    att_send,
    att_recv,
    need_send,
    need_recv,
    sum_send,
    sum_recv,
    blk_send,
    blk_recv,
):
    kz, ky, kc, x = (lax.axis_index(name) for name in KV_TP)
    me = kz * 8 + ky * 2 + kc

    def at(d):
        return (d // 8, lax.rem(d // 2, 4), lax.rem(d, 2), x)

    left, right, far = (lax.rem(x + hop, N_TP) for hop in (3, 1, 2))
    barrier = pltpu.get_barrier_semaphore()
    for peer in (left, right, far):
        pl.semaphore_signal(barrier, inc=1, device_id=(kz, ky, kc, peer), device_id_type=MESH)

    def greet(d, carry):
        @pl.when(d != me)
        def _():
            pl.semaphore_signal(barrier, inc=1, device_id=at(d), device_id_type=MESH)

        return carry

    lax.fori_loop(0, N_KV, greet, 0)

    loads = []

    def load(src, dst):
        loads.append(pltpu.make_async_copy(src, dst, load_sem.at[len(loads)]))
        loads[-1].start()
        return loads[-1]

    steps = D // CHUNK
    kv_loads = []
    for k in range(steps):
        rows = pl.ds(k * CHUNK, CHUNK)
        kv_loads.append(
            (
                load(wk_hbm.at[rows], wkv.at[rows, pl.ds(0, 128)]),
                load(wv_hbm.at[rows], wkv.at[rows, pl.ds(128, 128)]),
                load(tok_hbm.at[:, rows], tok.at[:, rows]),
            )
        )
    wg_load = load(wg_hbm, wg)
    wq_load = load(wq_hbm, wq)
    wo_load = load(wo_hbm, wall.at[pl.ds(pl.multiple_of(x * WIDTH, WIDTH), WIDTH)])
    make_plan(chosen_ref, need_ref, bias_ref)
    need_load = pltpu.make_async_copy(need_ref, need_s, load_sem.at[15])
    need_load.start()

    def clear(d, carry):
        sums[d] = jnp.zeros(sums.shape[1:], BF16)
        return carry

    lax.fori_loop(me + 1, N_KV, clear, 0)
    pl.semaphore_wait(barrier, N_KV - 1 + N_TP - 1)

    color = lax.rem(ky + kz, 2)
    mine_row = color * 256 + kc * 128
    other_row = (1 - color) * 256 + kc * 128

    def region(shard, row, count):
        return wall.at[pl.ds(pl.multiple_of(shard * WIDTH + row, 32), count)]

    def w_copy(index, src, dst, device):
        return pltpu.make_async_remote_copy(
            src_ref=src,
            dst_ref=dst,
            send_sem=w_send.at[index],
            recv_sem=w_recv.at[index],
            device_id=device,
            device_id_type=MESH,
        )

    def w_first(index, shard, receiving=False):
        to_right = index in (0, 1, 4)
        row = mine_row + (64 if index in (1, 2, 5) else 0)
        src = region(shard, row, 64)
        if index < 4 and not receiving:
            src = wo_hbm.at[pl.ds(pl.multiple_of(row, 32), 64)]
        device = (kz, ky, kc, right if to_right else left)
        return w_copy(index, src, region(shard, row, 64), device)

    directions = (
        (kz, lax.rem(ky + 1, 4), kc, x),
        (kz, lax.rem(ky + 3, 4), kc, x),
        (lax.rem(kz + 1, 4), ky, kc, x),
        (lax.rem(kz + 3, 4), ky, kc, x),
    )
    shards = (left, right, far)

    def w_second(j, o, receiving=False):
        part = region(shards[o], (other_row if receiving else mine_row) + 32 * j, 32)
        return w_copy(6 + 3 * j + o, part, part, directions[j])

    def w_third(half, o, receiving=False):
        row = mine_row if half == 0 else other_row
        row = row - kc * 128 + (1 - kc) * 128 if receiving else row
        part = region(shards[o], row, 128)
        return w_copy(18 + 3 * half + o, part, part, (kz, ky, 1 - kc, x))

    for index in (0, 2, 1, 3):
        w_first(index, x).start()

    def need_copy(d, sender):
        return pltpu.make_async_remote_copy(
            src_ref=need_ref.at[d],
            dst_ref=asked.at[sender],
            send_sem=need_send.at[d],
            recv_sem=need_recv.at[sender],
            device_id=at(d),
            device_id_type=MESH,
        )

    def send_need(d, carry):
        need_copy(d, me).start()
        return carry

    lax.fori_loop(0, me, send_need, 0)

    for k in range(steps):
        for copy in kv_loads[k]:
            copy.wait()
        part = nn_dot(tok[:, k * CHUNK : (k + 1) * CHUNK], wkv[k * CHUNK : (k + 1) * CHUNK])
        acc[...] = part if k == 0 else acc[...] + part
    low = lax.broadcasted_iota(jnp.int32, (ROWS, 128), 1) < HD
    keys = acc[:, :128].astype(BF16).astype(F32)
    values = acc[:, 128:].astype(BF16).astype(F32)
    pairs = (
        jnp.where(low, keys, pltpu.roll(values, HD, 1)),
        jnp.where(low, pltpu.roll(keys, HD, 1), values),
    )
    offsets = pos_ref[...].astype(F32)
    offsets = jnp.concatenate([offsets, offsets], axis=1)
    lane_low = lax.broadcasted_iota(jnp.int32, (CMP, 128), 1) < HD
    row_head = lax.broadcasted_iota(jnp.int32, (8, CMP), 0)
    diagonal = lax.broadcasted_iota(jnp.int32, (CMP, CMP), 0) == lax.broadcasted_iota(
        jnp.int32, (CMP, CMP), 1
    )

    def column(ref, head):
        row = jnp.sum(jnp.where(row_head == head, ref[...].astype(F32), 0.0), axis=0, keepdims=True)
        return jnp.sum(jnp.where(diagonal, row, 0.0), axis=1, keepdims=True)

    for g in range(GROUPS):
        pair = pairs[g]
        blocks = pair.astype(BF16).reshape(BLOCKS, SB, 128)
        mine[g] = blocks
        table[4 * N_KV + g * BLOCKS : 4 * N_KV + (g + 1) * BLOCKS] = blocks
        head = x * GROUPS + g
        mixing = jnp.where(lane_low, column(kmix_ref, head), column(vmix_ref, head))
        spans = jnp.sum((pair.reshape(SPANS, CMP, 128) + offsets[None]) * mixing[None], axis=1)
        sums[me, 0, g] = spans[:16].astype(BF16)
        sums[me, 1, g] = jnp.concatenate([spans[16:], jnp.zeros((12, 128), F32)], axis=0).astype(
            BF16
        )

    def sum_copy(d, sender):
        return pltpu.make_async_remote_copy(
            src_ref=sums.at[sender],
            dst_ref=sums.at[sender],
            send_sem=sum_send.at[d],
            recv_sem=sum_recv.at[sender],
            device_id=at(d),
            device_id_type=MESH,
        )

    def send_sum(d, carry):
        sum_copy(d, me).start()
        return carry

    lax.fori_loop(me + 1, N_KV, send_sum, 0)

    def take_need(d, carry):
        need_copy(me, d).wait_recv()
        copy = pltpu.make_async_copy(asked.at[d], asked_s.at[d], asked_sem.at[d])
        copy.start()
        return carry

    lax.fori_loop(me + 1, N_KV, take_need, 0)

    def blk_copy(d, sender):
        return pltpu.make_async_remote_copy(
            src_ref=stage.at[d],
            dst_ref=table.at[pl.ds(sender * 4, 4)],
            send_sem=blk_send.at[d],
            recv_sem=blk_recv.at[sender],
            device_id=at(d),
            device_id_type=MESH,
        )

    def send_blk(d, carry):
        pltpu.make_async_copy(asked.at[d], asked_s.at[d], asked_sem.at[d]).wait()
        for slot in range(4):
            block = asked_s[d, 0, slot]
            stage[d, slot] = mine[slot // 2, block]
        blk_copy(d, me).start()
        return carry

    lax.fori_loop(me + 1, N_KV, send_blk, 0)

    wq_load.wait()
    for g in range(GROUPS):
        cols = slice(256 * g, 256 * (g + 1))
        for k in range(steps):
            ks = slice(k * CHUNK, (k + 1) * CHUNK)
            part = nn_dot(tok[:, ks], wq[ks, cols])
            acc[...] = part if k == 0 else acc[...] + part
        for r in range(GROUP):
            tile = acc[:, 128 * (r // 2) : 128 * (r // 2) + 128]
            if r % 2:
                tile = pltpu.roll(tile, HD, 1)
            tile = jnp.where(low, tile, 0.0).astype(BF16) * BF16(HD**-0.5)
            qp[:, g, r] = tile.reshape(BLOCKS, SB, 128)
    wg_load.wait()
    pick = lax.broadcasted_iota(jnp.int32, (128, 64), 1) == (
        lax.broadcasted_iota(jnp.int32, (128, 64), 0) + x * 16
    )
    own_gates = nn_dot(jnp.where(pick, 1.0, 0.0).astype(BF16), wg[...]).astype(BF16)
    gates[...] = jax.nn.sigmoid(nt_dot(tok[...], own_gates)).reshape(BLOCKS, SB, 128)

    w_first(0, left, True).wait_recv()
    w_first(4, left).start()
    w_first(2, right, True).wait_recv()
    w_first(5, right).start()

    def take_sum(s, carry):
        sum_copy(me, s).wait_recv()
        return carry

    lax.fori_loop(0, me, take_sum, 0)
    lane_a = lax.broadcasted_iota(jnp.int32, (GROUP * SB, 512), 1)
    end_a = ((lane_a // 16) * SPANS + lax.rem(lane_a, 16)) * CMP + CMP - 1
    lane_b = lax.broadcasted_iota(jnp.int32, (GROUP * SB, 128), 1)
    end_b = ((lane_b // 4) * SPANS + 16 + lax.rem(lane_b, 4)) * CMP + CMP - 1
    row_a = lax.rem(lax.broadcasted_iota(jnp.int32, (GROUP * SB, 512), 0), SB)
    row_b = lax.rem(lax.broadcasted_iota(jnp.int32, (GROUP * SB, 128), 0), SB)
    row_c = lax.rem(lax.broadcasted_iota(jnp.int32, (GROUP * SB, 1), 0), SB)
    gap_a = end_a - row_a
    gap_b = end_b - row_b

    def gate_cols(b, g, branch):
        cols = [
            gates[b][:, 2 * (GROUP * g + r) + branch : 2 * (GROUP * g + r) + branch + 1]
            for r in range(GROUP)
        ]
        return jnp.concatenate(cols, axis=0)

    for g in range(GROUPS):
        span_a = sums[:, 0, g].reshape(N_KV * 16, 128)
        span_b = jnp.concatenate([sums[s, 1, g].astype(F32)[:4] for s in range(N_KV)], axis=0)
        span_b = span_b.astype(BF16)

        def compressed(b, carry):
            q = qp[b, g].reshape(GROUP * SB, 128)
            start = me * ROWS + b * SB
            score_a = jnp.where(gap_a <= start, nt_dot(q, span_a), LOW)
            score_b = jnp.where(gap_b <= start, nt_dot(q, span_b), LOW)
            most = jnp.maximum(
                jnp.max(score_a, axis=1, keepdims=True), jnp.max(score_b, axis=1, keepdims=True)
            )
            prob_a = jnp.exp(score_a - most)
            prob_b = jnp.exp(score_b - most)
            total = jnp.sum(prob_a, axis=1, keepdims=True) + jnp.sum(prob_b, axis=1, keepdims=True)
            mixed = nn_dot(prob_a.astype(BF16), span_a) + nn_dot(prob_b.astype(BF16), span_b)
            sees = row_c + start >= CMP - 1
            factor = jnp.where(sees, gate_cols(b, g, 0) / total, 0.0)
            comp[b, g] = mixed * factor
            return carry

        lax.fori_loop(0, BLOCKS, compressed, 0)

    def take_blk(s, carry):
        blk_copy(me, s).wait_recv()
        return carry

    lax.fori_loop(0, me, take_blk, 0)
    lane_first = lax.broadcasted_iota(jnp.int32, (GROUP * SB, 128), 1)
    causal = jnp.logical_or(lane_first >= SB, lane_first <= row_b)
    low_half = lax.broadcasted_iota(jnp.int32, (SB, 128), 1) < HD

    need_load.wait()
    for index, shard in ((1, left), (3, right), (4, far), (5, far)):
        w_first(index, shard, True).wait_recv()
    for o in range(3):
        for j in range(4):
            w_second(j, o).start()
    for o in range(3):
        w_third(0, o).start()

    def att_copy(target, sender):
        return pltpu.make_async_remote_copy(
            src_ref=att.at[pl.ds(pl.multiple_of(target * OUT_ROWS, 32), OUT_ROWS)],
            dst_ref=got.at[sender],
            send_sem=att_send.at[target],
            recv_sem=att_recv.at[sender],
            device_id=(kz, ky, kc, target),
            device_id_type=MESH,
        )

    first_block = lax.rem(5 * (x + 1) // 2, BLOCKS)

    def chosen_block(i, carry):
        b = lax.rem(first_block + i, BLOCKS)
        for g in range(GROUPS):
            q = qp[b, g].reshape(GROUP * SB, 128)
            pieces = []
            for s in range(N_SEL):
                named = chosen_s[b, g, s]
                source = named // BLOCKS
                place = named - source * BLOCKS
                second = (place != need_s[source, 0, 2 * g]).astype(jnp.int32)
                away = (source * GROUPS + g) * 2 + second
                home = 4 * N_KV + g * BLOCKS + place
                pieces.append(table[jnp.where(source == me, home, away)])
            picked = jnp.concatenate(pieces, axis=0)
            score = nt_dot(q, picked) + bias_ref[g, b]
            head = jnp.where(causal, score[:, :128], LOW)
            score = jnp.concatenate([head, score[:, 128:]], axis=1)
            most = jnp.max(score, axis=1, keepdims=True)
            prob = jnp.exp(score - most)
            total = jnp.sum(prob, axis=1, keepdims=True)
            mixed = nn_dot(prob.astype(BF16), picked)
            both = comp[b, g] + mixed * (gate_cols(b, g, 1) / total)
            for half in range(2):
                even = both[(2 * half) * SB : (2 * half + 1) * SB]
                odd = both[(2 * half + 1) * SB : (2 * half + 2) * SB]
                tile = jnp.where(low_half, pltpu.roll(even, HD, 1), odd).astype(BF16)
                lanes = slice(256 * g + 128 * half, 256 * g + 128 * half + 128)
                att[pl.ds(pl.multiple_of(b * SB, SB), SB), lanes] = tile
        for hop, last in ((1, 2), (2, 5), (3, 7)):

            @pl.when(i == last)
            def _():
                target = lax.rem(x + hop, N_TP)
                att_copy(target, x).start()

        return carry

    lax.fori_loop(0, BLOCKS, chosen_block, 0)
    for o in range(3):
        for j in range(4):
            w_second(j, o, True).wait_recv()
        w_third(1, o).start()

    wo_load.wait()
    got[x] = att[pl.ds(pl.multiple_of(x * OUT_ROWS, 32), OUT_ROWS)]
    for order, shard in enumerate((x, left, right, far)):
        if order:
            att_copy(shard, shard).wait_recv()
            w_third(0, order - 1, True).wait_recv()
            w_third(1, order - 1, True).wait_recv()

        def project(n, carry):
            cols = pl.ds(pl.multiple_of(n * 256, 256), 256)
            rows = pl.ds(pl.multiple_of(shard * WIDTH, WIDTH), WIDTH)
            part = nn_dot(got[shard], wall[rows, cols])
            if order:
                part = part + total_ref[:, cols]
            if order < 3:
                total_ref[:, cols] = part
            else:
                out_ref[:, cols] = part.astype(BF16)
            return carry

        lax.fori_loop(0, D // 256, project, 0)

    for index in (0, 1, 2, 3):
        w_first(index, x).wait_send()
    w_first(4, left).wait_send()
    w_first(5, right).wait_send()
    for o in range(3):
        for j in range(4):
            w_second(j, o).wait_send()
        w_third(0, o).wait_send()
        w_third(1, o).wait_send()
    for hop in (1, 2, 3):
        att_copy(lax.rem(x + hop, N_TP), x).wait_send()

    def sent_need(d, carry):
        need_copy(d, me).wait_send()
        return carry

    lax.fori_loop(0, me, sent_need, 0)

    def sent_rest(d, carry):
        sum_copy(d, me).wait_send()
        blk_copy(d, me).wait_send()
        return carry

    lax.fori_loop(me + 1, N_KV, sent_rest, 0)


def local(
    tokens,
    query_weight,
    key_weight,
    value_weight,
    gate_weight,
    summary_pos,
    key_mixing,
    value_mixing,
    out_weight,
    chosen,
):
    any_space = pl.BlockSpec(memory_space=pl.ANY)
    vmem = pl.BlockSpec(memory_space=pltpu.VMEM)
    smem = pl.BlockSpec(memory_space=pltpu.SMEM)
    dma = pltpu.SemaphoreType.DMA
    return pl.pallas_call(
        body,
        out_shape=jax.ShapeDtypeStruct((OUT_ROWS, D), BF16),
        in_specs=[any_space] * 5 + [vmem] * 3 + [any_space, vmem, smem],
        out_specs=vmem,
        scratch_shapes=[
            pltpu.VMEM((ROWS, D), BF16),
            pltpu.VMEM((D, WIDTH), BF16),
            pltpu.VMEM((D, 256), BF16),
            pltpu.VMEM((64, D), BF16),
            pltpu.VMEM((ROWS, 256), F32),
            pltpu.VMEM((BLOCKS, SB, 128), F32),
            pltpu.VMEM((BLOCKS, GROUPS, GROUP, SB, 128), BF16),
            pltpu.VMEM((N_KV, 2, GROUPS, 16, 128), BF16),
            pltpu.VMEM((N_KV, 1, 128), jnp.int32),
            pltpu.SMEM((N_KV, 1, 128), jnp.int32),
            pltpu.VMEM((4 * N_KV + GROUPS * BLOCKS, SB, 128), BF16),
            pltpu.VMEM((N_KV, 4, SB, 128), BF16),
            pltpu.VMEM((GROUPS, BLOCKS, SB, 128), BF16),
            pltpu.VMEM((BLOCKS, GROUPS, GROUP * SB, 128), F32),
            pltpu.VMEM((N_KV, 1, 128), jnp.int32),
            pltpu.SMEM((N_KV, 1, 128), jnp.int32),
            pltpu.VMEM((GROUPS, BLOCKS, 1, N_SEL * SB), F32),
            pltpu.VMEM((N_TP * WIDTH, D), BF16),
            pltpu.VMEM((ROWS, WIDTH), BF16),
            pltpu.VMEM((N_TP, OUT_ROWS, WIDTH), BF16),
            pltpu.VMEM((OUT_ROWS, D), F32),
            dma((16,)),
            dma((N_KV,)),
            dma((24,)),
            dma((24,)),
            dma((N_TP,)),
            dma((N_TP,)),
            dma((N_KV,)),
            dma((N_KV,)),
            dma((N_KV,)),
            dma((N_KV,)),
            dma((N_KV,)),
            dma((N_KV,)),
        ],
        compiler_params=pltpu.CompilerParams(
            collective_id=0, has_side_effects=True, vmem_limit_bytes=63 * 1024 * 1024
        ),
    )(
        tokens,
        query_weight,
        key_weight,
        value_weight,
        gate_weight.T,
        summary_pos,
        key_mixing.T,
        value_mixing.T,
        out_weight,
        chosen,
        chosen,
    )


def solution(mesh):
    torus = Mesh(mesh.devices.reshape(4, 4, 2, mesh.shape["tp"]), ("kv_0", "kv_1", "kv_2", "tp"))
    in_specs = (
        P(KV, None),
        P(None, "tp"),
        P(None, "tp"),
        P(None, "tp"),
        P(),
        P(),
        P(),
        P(),
        P("tp", None),
        P(KV, "tp", None),
    )
    out_specs = P(KV_TP, None)
    return jax.shard_map(local, mesh=torus, in_specs=in_specs, out_specs=out_specs, check_vma=False)
```

```python
import jax
import jax.numpy as jnp
from jax import lax
from jax.experimental import pallas as pl
from jax.experimental.pallas import tpu as pltpu
from jax.sharding import Mesh
from jax.sharding import PartitionSpec as P

HD = 64
CMP = 32
SB = 64
N_SEL = 16
N_KV = 32
N_Z = 4
PLANE = 8
N_TP = 4
ROWS = 640
BLOCKS = 10
GROUPS = 2
GROUP = 4
SPANS = 20
WIDTH = 512
OUT_ROWS = 160
D = 4096
CHUNK = 1024
KV = ("kv_0", "kv_1", "kv_2")
KV_TP = ("kv_0", "kv_1", "kv_2", "tp")
MESH = pl.DeviceIdType.MESH
BF16 = jnp.bfloat16
F32 = jnp.float32
LOW = -1e30


def nt_dot(a, b):
    return lax.dot_general(a, b, (((1,), (1,)), ((), ())), preferred_element_type=F32)


def nn_dot(a, b):
    return jnp.dot(a, b, preferred_element_type=F32)


def make_plan(chosen_ref, need_ref, bias_ref):
    lane = lax.broadcasted_iota(jnp.int32, (BLOCKS, N_SEL), 1)
    spread = lax.broadcasted_iota(jnp.int32, (N_SEL, N_SEL * SB), 1) // SB
    spread = spread == lax.broadcasted_iota(jnp.int32, (N_SEL, N_SEL * SB), 0)
    spread = jnp.where(spread, 1.0, 0.0).astype(BF16)
    need_lane = lax.broadcasted_iota(jnp.int32, (1, 128), 1)
    named = [chosen_ref[:, g, :] for g in range(GROUPS)]
    for g in range(GROUPS):
        repeated = jnp.zeros((BLOCKS, N_SEL), F32)
        for t in range(N_SEL - 1):
            same = jnp.logical_and(named[g] == named[g][:, t : t + 1], lane > t)
            repeated = jnp.where(same, 1.0, repeated)
        bias = nn_dot(repeated.astype(BF16), spread) * LOW
        for b in range(BLOCKS):
            bias_ref[g, b] = bias[b : b + 1]
    places = [n - (n // BLOCKS) * BLOCKS for n in named]
    sources = [n // BLOCKS for n in named]

    def ends(axis_min, value):
        for axis in (0, 1):
            value = axis_min(value, axis=axis, keepdims=True)
        return value

    for s in range(N_KV):
        row = jnp.zeros((1, 128), jnp.int32)
        for g in range(GROUPS):
            hit = sources[g] == s
            first = ends(jnp.min, jnp.where(hit, places[g], BLOCKS - 1))
            last = ends(jnp.max, jnp.where(hit, places[g], 0))
            row = jnp.where(need_lane == 2 * g, first, row)
            row = jnp.where(need_lane == 2 * g + 1, last, row)
        need_ref[s // PLANE, s % PLANE] = row


def body(
    tok_hbm,
    wq_hbm,
    wk_hbm,
    wv_hbm,
    wg_hbm,
    pos_ref,
    kmix_ref,
    vmix_ref,
    wo_hbm,
    chosen_ref,
    chosen_s,
    out_ref,
    tok,
    wq,
    wkv,
    wg,
    acc,
    gates,
    qp,
    sums,
    asked,
    asked_s,
    table,
    stage,
    unit_0,
    unit_1,
    unit_2,
    unit_3,
    comp,
    need_ref,
    need_s,
    bias_ref,
    wall,
    att,
    got,
    load_sem,
    asked_sem,
    w_send,
    w_recv,
    att_send,
    att_recv,
    need_send,
    need_recv,
    lift_send,
    lift_recv,
    unit_send,
    unit_recv,
    sum_send,
    sum_recv,
    blk_send,
    blk_recv,
):
    kz, ky, kc, x = (lax.axis_index(name) for name in KV_TP)
    kp = ky * 2 + kc
    me = kz * PLANE + kp
    units = (unit_0, unit_1, unit_2, unit_3)

    def in_plane(p):
        return (kz, p // 2, lax.rem(p, 2), x)

    def above(hops):
        return (lax.rem(kz + hops, N_Z), ky, kc, x)

    left, right, far = (lax.rem(x + hop, N_TP) for hop in (3, 1, 2))
    barrier = pltpu.get_barrier_semaphore()

    def signal(device):
        pl.semaphore_signal(barrier, inc=1, device_id=device, device_id_type=MESH)

    for peer in (left, right, far):
        signal((kz, ky, kc, peer))
    for hops in (1, 2, 3):
        signal(above(hops))
    for hop in range(1, PLANE):
        signal(in_plane(lax.rem(kp + hop, PLANE)))

    loads = []

    def load(src, dst):
        loads.append(pltpu.make_async_copy(src, dst, load_sem.at[len(loads)]))
        loads[-1].start()
        return loads[-1]

    steps = D // CHUNK
    kv_loads = []
    for k in range(steps):
        rows = pl.ds(k * CHUNK, CHUNK)
        kv_loads.append(
            (
                load(wk_hbm.at[rows], wkv.at[rows, pl.ds(0, 128)]),
                load(wv_hbm.at[rows], wkv.at[rows, pl.ds(128, 128)]),
                load(tok_hbm.at[:, rows], tok.at[:, rows]),
            )
        )
    wq_load = load(wq_hbm, wq)
    wg_load = load(wg_hbm, wg.at[pl.ds(0, 64)])
    wo_load = load(wo_hbm, wall.at[pl.ds(pl.multiple_of(x * WIDTH, WIDTH), WIDTH)])
    with jax.named_scope("plan"):
        make_plan(chosen_ref, need_ref, bias_ref)
        need_load = pltpu.make_async_copy(need_ref, need_s, load_sem.at[15])
        need_load.start()
    wg[64:] = jnp.zeros((64, D), BF16)

    def clear(d, carry):
        sums[d // PLANE, lax.rem(d, PLANE)] = jnp.zeros(sums.shape[2:], BF16)
        return carry

    lax.fori_loop(me + 1, N_KV, clear, 0)
    with jax.named_scope("barrier_wait"):
        pl.semaphore_wait(barrier, PLANE - 1 + N_Z - 1 + N_TP - 1)

    def remote(src, dst, send, recv, device):
        return pltpu.make_async_remote_copy(
            src_ref=src,
            dst_ref=dst,
            send_sem=send,
            recv_sem=recv,
            device_id=device,
            device_id_type=MESH,
        )

    def need_copy(p, sender):
        return remote(
            need_ref.at[:, p], asked.at[sender], need_send.at[p], need_recv.at[sender], in_plane(p)
        )

    def peers(fn):
        def step(p, carry):
            @pl.when(p != kp)
            def _():
                fn(p)

            return carry

        lax.fori_loop(0, PLANE, step, 0)

    peers(lambda p: need_copy(p, kp).start())

    color = lax.rem(ky + kz, 2)
    mine_row = color * 256 + kc * 128
    other_row = (1 - color) * 256 + kc * 128

    def region(shard, row, count):
        return wall.at[pl.ds(pl.multiple_of(shard * WIDTH + row, 32), count)]

    def w_copy(index, src, dst, device):
        return remote(src, dst, w_send.at[index], w_recv.at[index], device)

    def w_first(index, shard, receiving=False):
        to_right = index in (0, 1, 4)
        row = mine_row + (64 if index in (1, 2, 5) else 0)
        src = region(shard, row, 64)
        if index < 4 and not receiving:
            src = wo_hbm.at[pl.ds(pl.multiple_of(row, 32), 64)]
        device = (kz, ky, kc, right if to_right else left)
        return w_copy(index, src, region(shard, row, 64), device)

    directions = (
        (kz, lax.rem(ky + 1, 4), kc, x),
        (kz, lax.rem(ky + 3, 4), kc, x),
        (lax.rem(kz + 1, 4), ky, kc, x),
        (lax.rem(kz + 3, 4), ky, kc, x),
    )
    shards = (left, right, far)

    def w_second(j, o, receiving=False):
        part = region(shards[o], (other_row if receiving else mine_row) + 32 * j, 32)
        return w_copy(6 + 3 * j + o, part, part, directions[j])

    def w_third(half, o, receiving=False):
        row = mine_row if half == 0 else other_row
        row = row - kc * 128 + (1 - kc) * 128 if receiving else row
        part = region(shards[o], row, 128)
        return w_copy(18 + 3 * half + o, part, part, (kz, ky, 1 - kc, x))

    for index in (0, 2, 1, 3):
        w_first(index, x).start()

    with jax.named_scope("kv_proj"):
        for k in range(steps):
            for copy in kv_loads[k]:
                copy.wait()
            part = nn_dot(tok[:, k * CHUNK : (k + 1) * CHUNK], wkv[k * CHUNK : (k + 1) * CHUNK])
            acc[...] = part if k == 0 else acc[...] + part
    low = lax.broadcasted_iota(jnp.int32, (ROWS, 128), 1) < HD
    keys = acc[:, :128].astype(BF16).astype(F32)
    values = acc[:, 128:].astype(BF16).astype(F32)
    pairs = (
        jnp.where(low, keys, pltpu.roll(values, HD, 1)),
        jnp.where(low, pltpu.roll(keys, HD, 1), values),
    )
    offsets = pos_ref[...].astype(F32)
    offsets = jnp.concatenate([offsets, offsets], axis=1)
    lane_low = lax.broadcasted_iota(jnp.int32, (CMP, 128), 1) < HD
    row_head = lax.broadcasted_iota(jnp.int32, (8, CMP), 0)
    diagonal = lax.broadcasted_iota(jnp.int32, (CMP, CMP), 0) == lax.broadcasted_iota(
        jnp.int32, (CMP, CMP), 1
    )

    def column(ref, head):
        row = jnp.sum(jnp.where(row_head == head, ref[...].astype(F32), 0.0), axis=0, keepdims=True)
        return jnp.sum(jnp.where(diagonal, row, 0.0), axis=1, keepdims=True)

    with jax.named_scope("summary"):
        tails = []
        for g in range(GROUPS):
            pair = pairs[g]
            blocks = pair.astype(BF16).reshape(BLOCKS, SB, 128)
            unit_0[g] = blocks
            table[4 * N_KV + g * BLOCKS : 4 * N_KV + (g + 1) * BLOCKS] = blocks
            head = x * GROUPS + g
            mixing = jnp.where(lane_low, column(kmix_ref, head), column(vmix_ref, head))
            spans = jnp.sum((pair.reshape(SPANS, CMP, 128) + offsets[None]) * mixing[None], axis=1)
            sums[kz, kp, 16 * g : 16 * g + 16] = spans[:16].astype(BF16)
            tails.append(spans[16:])
        sums[kz, kp, 32:] = jnp.concatenate(tails, axis=0).astype(BF16)

    def lift_copy(hops, receiving=False):
        part = sums.at[kz - hops if receiving else kz, kp]
        return remote(part, part, lift_send.at[hops], lift_recv.at[hops], above(hops))

    def sum_copy(hops, p, sender):
        part = sums.at[kz - hops, sender]
        k = hops * PLANE
        return remote(part, part, sum_send.at[k + p], sum_recv.at[k + sender], in_plane(p))

    def spread(hops, fn):
        def step(p, carry):
            @pl.when(p > kp if hops == 0 else p != kp)
            def _():
                fn(p)

            return carry

        lax.fori_loop(0, PLANE, step, 0)

    def arriving(hops, fn):
        def step(p, carry):
            @pl.when(p < kp if hops == 0 else p != kp)
            def _():
                fn(p)

            return carry

        lax.fori_loop(0, PLANE, step, 0)

    for hops in (1, 2, 3):

        @pl.when(kz + hops < N_Z)
        def _():
            lift_copy(hops).start()

    spread(0, lambda p: sum_copy(0, p, kp).start())

    def unit_copy(hops):
        src = unit_0 if hops in (1, 3) else unit_1
        device = above(3 if hops == 3 else 1)
        return remote(src, units[hops], unit_send.at[hops], unit_recv.at[hops], device)

    sends_unit = {1: kz < 3, 2: jnp.logical_or(kz == 1, kz == 2), 3: kz == 0}
    for hops in (1, 3):

        @pl.when(sends_unit[hops])
        def _():
            unit_copy(hops).start()

    with jax.named_scope("need_wait"):

        def take_need(p):
            need_copy(kp, p).wait_recv()
            pltpu.make_async_copy(asked.at[p], asked_s.at[p], asked_sem.at[p]).start()

        peers(take_need)
        peers(lambda p: pltpu.make_async_copy(asked.at[p], asked_s.at[p], asked_sem.at[p]).wait())
        need_load.wait()

    def blk_copy(hops, p, sender):
        dst = table.at[pl.ds(((kz - hops) * PLANE + sender) * 4, 4)]
        k = hops * PLANE
        return remote(
            stage.at[hops, p], dst, blk_send.at[k + p], blk_recv.at[k + sender], in_plane(p)
        )

    def serve(hops):
        @pl.when(kz >= hops)
        def _():
            if hops:
                unit_copy(hops).wait_recv()
            if hops == 1:

                @pl.when(sends_unit[2])
                def _():
                    unit_copy(2).start()

            def one(p):
                for slot in range(4):
                    block = asked_s[p, kz - hops, 0, slot]
                    stage[hops, p, slot] = units[hops][slot // 2, block]
                blk_copy(hops, p, kp).start()

            spread(hops, one)
            if hops:
                for slot in range(4):
                    block = need_s[kz - hops, kp, 0, slot]
                    place = ((kz - hops) * PLANE + kp) * 4 + slot
                    table[place] = units[hops][slot // 2, block]

    with jax.named_scope("serve_0"):
        serve(0)

    def project_queries(g):
        cols = slice(256 * g, 256 * (g + 1))
        for k in range(steps):
            ks = slice(k * CHUNK, (k + 1) * CHUNK)
            part = nn_dot(tok[:, ks], wq[ks, cols])
            acc[...] = part if k == 0 else acc[...] + part
        for r in range(GROUP):
            tile = acc[:, 128 * (r // 2) : 128 * (r // 2) + 128]
            if r % 2:
                tile = pltpu.roll(tile, HD, 1)
            tile = jnp.where(low, tile, 0.0).astype(BF16) * BF16(HD**-0.5)
            qp[:, g, r] = tile.reshape(BLOCKS, SB, 128)

    with jax.named_scope("q_proj"):
        wq_load.wait()
        project_queries(0)
    with jax.named_scope("sum_pass"):
        for hops in (1, 2, 3):

            @pl.when(kz >= hops)
            def _():
                lift_copy(hops, True).wait_recv()
                spread(hops, lambda p: sum_copy(hops, p, kp).start())

    with jax.named_scope("q_proj"):
        project_queries(1)
    with jax.named_scope("gates"):
        wg_load.wait()
        logits = nt_dot(tok[...], wg[...])
        own = pltpu.roll(logits, lax.rem(128 - x * 16, 128), 1)
        gates[...] = jax.nn.sigmoid(own).reshape(BLOCKS, SB, 128)

    with jax.named_scope("sum_wait"):
        for hops in range(N_Z):

            @pl.when(kz >= hops)
            def _():
                arriving(hops, lambda p: sum_copy(hops, kp, p).wait_recv())

    lane_a = lax.broadcasted_iota(jnp.int32, (GROUP * SB, 512), 1)
    end_a = ((lane_a // 16) * SPANS + lax.rem(lane_a, 16)) * CMP + CMP - 1
    lane_b = lax.broadcasted_iota(jnp.int32, (GROUP * SB, 128), 1)
    end_b = ((lane_b // 4) * SPANS + 16 + lax.rem(lane_b, 4)) * CMP + CMP - 1
    row_a = lax.rem(lax.broadcasted_iota(jnp.int32, (GROUP * SB, 512), 0), SB)
    row_b = lax.rem(lax.broadcasted_iota(jnp.int32, (GROUP * SB, 128), 0), SB)
    row_c = lax.rem(lax.broadcasted_iota(jnp.int32, (GROUP * SB, 1), 0), SB)
    gap_a = end_a - row_a
    gap_b = end_b - row_b

    def gate_cols(b, g, branch):
        cols = [
            gates[b][:, 2 * (GROUP * g + r) + branch : 2 * (GROUP * g + r) + branch + 1]
            for r in range(GROUP)
        ]
        return jnp.concatenate(cols, axis=0)

    span_as = [sums[:, :, 16 * g : 16 * g + 16].reshape(N_KV * 16, 128) for g in range(GROUPS)]
    span_bs = []
    for g in range(GROUPS):
        tails = [
            sums[s // PLANE, s % PLANE, 32:].astype(F32)[4 * g : 4 * g + 4] for s in range(N_KV)
        ]
        span_bs.append(jnp.concatenate(tails, axis=0).astype(BF16))

    def compressed(b, carry):
        start = me * ROWS + b * SB
        for g in range(GROUPS):
            span_a, span_b = span_as[g], span_bs[g]
            q = qp[b, g].reshape(GROUP * SB, 128)
            score_a = jnp.where(gap_a <= start, nt_dot(q, span_a), LOW)
            score_b = jnp.where(gap_b <= start, nt_dot(q, span_b), LOW)
            most = jnp.maximum(
                jnp.max(score_a, axis=1, keepdims=True), jnp.max(score_b, axis=1, keepdims=True)
            )
            prob_a = jnp.exp(score_a - most)
            prob_b = jnp.exp(score_b - most)
            total = jnp.sum(prob_a, axis=1, keepdims=True) + jnp.sum(prob_b, axis=1, keepdims=True)
            mixed = nn_dot(prob_a.astype(BF16), span_a) + nn_dot(prob_b.astype(BF16), span_b)
            sees = row_c + start >= CMP - 1
            factor = jnp.where(sees, gate_cols(b, g, 0) / total, 0.0)
            comp[b, g] = mixed * factor

        @pl.when(b == 0)
        def _():
            with jax.named_scope("serve_1"):
                serve(1)

        @pl.when(b == 1)
        def _():
            with jax.named_scope("relay"):
                w_first(0, left, True).wait_recv()
                w_first(4, left).start()
                w_first(2, right, True).wait_recv()
                w_first(5, right).start()
            with jax.named_scope("serve_3"):
                serve(3)

        @pl.when(b == 6)
        def _():
            with jax.named_scope("serve_2"):
                serve(2)

        return carry

    with jax.named_scope("comp"):
        lax.fori_loop(0, BLOCKS, compressed, 0)

    with jax.named_scope("w1_wait"):
        w_first(1, left, True).wait_recv()
        w_first(3, right, True).wait_recv()
        for o in range(2):
            for j in range(4):
                w_second(j, o).start()
            w_third(0, o).start()
    with jax.named_scope("blk_wait"):
        for hops in range(N_Z):

            @pl.when(kz >= hops)
            def _():
                arriving(hops, lambda p: blk_copy(hops, kp, p).wait_recv())

    lane_first = lax.broadcasted_iota(jnp.int32, (GROUP * SB, 128), 1)
    causal = jnp.logical_or(lane_first >= SB, lane_first <= row_b)
    low_half = lax.broadcasted_iota(jnp.int32, (SB, 128), 1) < HD

    def att_copy(target, sender):
        rows = pl.ds(pl.multiple_of(target * OUT_ROWS, 32), OUT_ROWS)
        return remote(
            att.at[rows],
            got.at[sender],
            att_send.at[target],
            att_recv.at[sender],
            (kz, ky, kc, target),
        )

    first_block = lax.rem(5 * (x + 1) // 2, BLOCKS)

    def chosen_block(i, carry):
        b = lax.rem(first_block + i, BLOCKS)
        for g in range(GROUPS):
            q = qp[b, g].reshape(GROUP * SB, 128)
            pieces = []
            for s in range(N_SEL):
                named = chosen_s[b, g, s]
                source = named // BLOCKS
                place = named - source * BLOCKS
                first = need_s[source // PLANE, lax.rem(source, PLANE), 0, 2 * g]
                away = (source * GROUPS + g) * 2 + (place != first).astype(jnp.int32)
                home = 4 * N_KV + g * BLOCKS + place
                pieces.append(table[jnp.where(source == me, home, away)])
            picked = jnp.concatenate(pieces, axis=0)
            score = nt_dot(q, picked) + bias_ref[g, b]
            head = jnp.where(causal, score[:, :128], LOW)
            score = jnp.concatenate([head, score[:, 128:]], axis=1)
            most = jnp.max(score, axis=1, keepdims=True)
            prob = jnp.exp(score - most)
            total = jnp.sum(prob, axis=1, keepdims=True)
            mixed = nn_dot(prob.astype(BF16), picked)
            both = comp[b, g] + mixed * (gate_cols(b, g, 1) / total)
            for half in range(2):
                even = both[(2 * half) * SB : (2 * half + 1) * SB]
                odd = both[(2 * half + 1) * SB : (2 * half + 2) * SB]
                tile = jnp.where(low_half, pltpu.roll(even, HD, 1), odd).astype(BF16)
                lanes = slice(256 * g + 128 * half, 256 * g + 128 * half + 128)
                att[pl.ds(pl.multiple_of(b * SB, SB), SB), lanes] = tile
        for hop, last in ((1, 2), (2, 5), (3, 7)):

            @pl.when(i == last)
            def _():
                target = lax.rem(x + hop, N_TP)
                att_copy(target, x).start()

        @pl.when(i == 4)
        def _():
            with jax.named_scope("w1_far"):
                w_first(4, far, True).wait_recv()
                w_first(5, far, True).wait_recv()
                for j in range(4):
                    w_second(j, 2).start()
                w_third(0, 2).start()

        @pl.when(i == 8)
        def _():
            with jax.named_scope("w2_near"):
                for o in range(2):
                    for j in range(4):
                        w_second(j, o, True).wait_recv()
                    w_third(1, o).start()

        return carry

    with jax.named_scope("chosen"):
        lax.fori_loop(0, BLOCKS, chosen_block, 0)

    with jax.named_scope("wo_wait"):
        wo_load.wait()
    got[x] = att[pl.ds(pl.multiple_of(x * OUT_ROWS, 32), OUT_ROWS)]
    for order, shard in enumerate((x, left, right, far)):
        if order:
            with jax.named_scope("w3_wait"):
                att_copy(shard, shard).wait_recv()
                w_third(0, order - 1, True).wait_recv()
                w_third(1, order - 1, True).wait_recv()

        def project(n, carry):
            cols = pl.ds(pl.multiple_of(n * CHUNK, CHUNK), CHUNK)
            rows = pl.ds(pl.multiple_of(shard * WIDTH, WIDTH), WIDTH)
            part = nn_dot(got[shard], wall[rows, cols])
            out_ref[:, cols] = part + out_ref[:, cols] if order else part
            return carry

        with jax.named_scope("outproj"):
            lax.fori_loop(0, D // CHUNK, project, 0)
        if order == 0:
            with jax.named_scope("w2_far"):
                for j in range(4):
                    w_second(j, 2, True).wait_recv()
                w_third(1, 2).start()

    with jax.named_scope("drain"):
        peers(lambda p: need_copy(p, kp).wait_send())
        for index in (0, 1, 2, 3):
            w_first(index, x).wait_send()
        w_first(4, left).wait_send()
        w_first(5, right).wait_send()
        for o in range(3):
            for j in range(4):
                w_second(j, o).wait_send()
            w_third(0, o).wait_send()
            w_third(1, o).wait_send()
        for hop in (1, 2, 3):
            att_copy(lax.rem(x + hop, N_TP), x).wait_send()
        for hops in (1, 2, 3):

            @pl.when(kz + hops < N_Z)
            def _():
                lift_copy(hops).wait_send()

            @pl.when(sends_unit[hops])
            def _():
                unit_copy(hops).wait_send()

        for hops in range(N_Z):

            @pl.when(kz >= hops)
            def _():
                def done(p):
                    sum_copy(hops, p, kp).wait_send()
                    blk_copy(hops, p, kp).wait_send()

                spread(hops, done)


def local(
    tokens,
    query_weight,
    key_weight,
    value_weight,
    gate_weight,
    summary_pos,
    key_mixing,
    value_mixing,
    out_weight,
    chosen,
):
    any_space = pl.BlockSpec(memory_space=pl.ANY)
    vmem = pl.BlockSpec(memory_space=pltpu.VMEM)
    smem = pl.BlockSpec(memory_space=pltpu.SMEM)
    dma = pltpu.SemaphoreType.DMA
    unit = pltpu.VMEM((GROUPS, BLOCKS, SB, 128), BF16)
    requests = (N_Z, PLANE, 1, 128)
    total = pl.pallas_call(
        body,
        out_shape=jax.ShapeDtypeStruct((OUT_ROWS, D), F32),
        in_specs=[any_space] * 5 + [vmem] * 3 + [any_space, vmem, smem],
        out_specs=vmem,
        scratch_shapes=[
            pltpu.VMEM((ROWS, D), BF16),
            pltpu.VMEM((D, WIDTH), BF16),
            pltpu.VMEM((D, 256), BF16),
            pltpu.VMEM((128, D), BF16),
            pltpu.VMEM((ROWS, 256), F32),
            pltpu.VMEM((BLOCKS, SB, 128), F32),
            pltpu.VMEM((BLOCKS, GROUPS, GROUP, SB, 128), BF16),
            pltpu.VMEM((N_Z, PLANE, 40, 128), BF16),
            pltpu.VMEM((PLANE, N_Z, 1, 128), jnp.int32),
            pltpu.SMEM((PLANE, N_Z, 1, 128), jnp.int32),
            pltpu.VMEM((4 * N_KV + GROUPS * BLOCKS, SB, 128), BF16),
            pltpu.VMEM((N_Z, PLANE, 4, SB, 128), BF16),
            unit,
            unit,
            unit,
            unit,
            pltpu.VMEM((BLOCKS, GROUPS, GROUP * SB, 128), F32),
            pltpu.VMEM(requests, jnp.int32),
            pltpu.SMEM(requests, jnp.int32),
            pltpu.VMEM((GROUPS, BLOCKS, 1, N_SEL * SB), F32),
            pltpu.VMEM((N_TP * WIDTH, D), BF16),
            pltpu.VMEM((ROWS, WIDTH), BF16),
            pltpu.VMEM((N_TP, OUT_ROWS, WIDTH), BF16),
            dma((16,)),
            dma((PLANE,)),
            dma((24,)),
            dma((24,)),
            dma((N_TP,)),
            dma((N_TP,)),
            dma((PLANE,)),
            dma((PLANE,)),
            dma((N_Z,)),
            dma((N_Z,)),
            dma((N_Z,)),
            dma((N_Z,)),
            dma((N_KV,)),
            dma((N_KV,)),
            dma((N_KV,)),
            dma((N_KV,)),
        ],
        compiler_params=pltpu.CompilerParams(
            collective_id=0, has_side_effects=True, vmem_limit_bytes=60 * 1024 * 1024
        ),
    )(
        tokens,
        query_weight,
        key_weight,
        value_weight,
        gate_weight.T,
        summary_pos,
        key_mixing.T,
        value_mixing.T,
        out_weight,
        chosen,
        chosen,
    )
    return total.astype(BF16)


def solution(mesh):
    torus = Mesh(mesh.devices.reshape(4, 4, 2, mesh.shape["tp"]), ("kv_0", "kv_1", "kv_2", "tp"))
    in_specs = (
        P(KV, None),
        P(None, "tp"),
        P(None, "tp"),
        P(None, "tp"),
        P(),
        P(),
        P(),
        P(),
        P("tp", None),
        P(KV, "tp", None),
    )
    out_specs = P(KV_TP, None)
    return jax.shard_map(local, mesh=torus, in_specs=in_specs, out_specs=out_specs, check_vma=False)
```

```python
import jax
import jax.numpy as jnp
from jax import lax
from jax.experimental import pallas as pl
from jax.experimental.pallas import tpu as pltpu
from jax.sharding import Mesh
from jax.sharding import PartitionSpec as P

HD = 64
CMP = 32
SB = 64
N_SEL = 16
N_KV = 32
N_Z = 4
PLANE = 8
N_TP = 4
ROWS = 640
BLOCKS = 10
GROUPS = 2
GROUP = 4
SPANS = 20
N_SPANS = 640
VMEM_MIB = 58
STRIP = 32
HALVES = (slice(0, 320), slice(320, 640))
WIDTH = 512
OUT_ROWS = 160
D = 4096
CHUNK = 1024
KV = ("kv_0", "kv_1", "kv_2")
KV_TP = ("kv_0", "kv_1", "kv_2", "tp")
MESH = pl.DeviceIdType.MESH
BF16 = jnp.bfloat16
F32 = jnp.float32
LOW = -1e30


def nt_dot(a, b):
    return lax.dot_general(a, b, (((1,), (1,)), ((), ())), preferred_element_type=F32)


def nn_dot(a, b):
    return jnp.dot(a, b, preferred_element_type=F32)


def make_plan(me, chosen_ref, need_ref, index_ref, bias_ref):
    lane = lax.broadcasted_iota(jnp.int32, (BLOCKS, N_SEL), 1)
    spread = lax.broadcasted_iota(jnp.int32, (N_SEL, N_SEL * SB), 1) // SB
    spread = spread == lax.broadcasted_iota(jnp.int32, (N_SEL, N_SEL * SB), 0)
    spread = jnp.where(spread, 1.0, 0.0).astype(BF16)
    need_lane = lax.broadcasted_iota(jnp.int32, (1, 128), 1)
    named = [chosen_ref[:, g, :] for g in range(GROUPS)]
    for g in range(GROUPS):
        repeated = jnp.zeros((BLOCKS, N_SEL), F32)
        for t in range(N_SEL - 1):
            same = jnp.logical_and(named[g] == named[g][:, t : t + 1], lane > t)
            repeated = jnp.where(same, 1.0, repeated)
        bias = nn_dot(repeated.astype(BF16), spread) * LOW
        for b in range(BLOCKS):
            bias_ref[g, b] = bias[b : b + 1]
    places = [n - (n // BLOCKS) * BLOCKS for n in named]
    sources = [n // BLOCKS for n in named]

    def ends(axis_min, value):
        for axis in (0, 1):
            value = axis_min(value, axis=axis, keepdims=True)
        return value

    firsts = [jnp.zeros((BLOCKS, N_SEL), jnp.int32) for _ in range(GROUPS)]
    for s in range(N_KV):
        row = jnp.zeros((1, 128), jnp.int32)
        for g in range(GROUPS):
            hit = sources[g] == s
            first = ends(jnp.min, jnp.where(hit, places[g], BLOCKS - 1))
            last = ends(jnp.max, jnp.where(hit, places[g], 0))
            firsts[g] = jnp.where(hit, first, firsts[g])
            row = jnp.where(need_lane == 2 * g, first, row)
            row = jnp.where(need_lane == 2 * g + 1, last, row)
        need_ref[s // PLANE, s % PLANE] = row
    for g in range(GROUPS):
        away = (sources[g] * GROUPS + g) * 2 + jnp.where(places[g] == firsts[g], 0, 1)
        home = 4 * N_KV + g * BLOCKS + places[g]
        index_ref[g, :BLOCKS, :N_SEL] = jnp.where(sources[g] == me, home, away)


def body(
    tok_hbm,
    wq_hbm,
    wk_hbm,
    wv_hbm,
    wg_hbm,
    pos_ref,
    kmix_ref,
    vmix_ref,
    wo_hbm,
    chosen_ref,
    out_ref,
    tok,
    wq,
    wkv,
    wg,
    acc,
    gates,
    qp,
    sums,
    asked,
    asked_s,
    asked_far,
    asked_far_s,
    table,
    stage,
    unit_0,
    unit_1,
    unit_2,
    comp,
    score,
    prob,
    keys_in,
    values_in,
    span_keys,
    span_values,
    mask,
    need_ref,
    need_s,
    index_ref,
    index_s,
    bias_ref,
    wall,
    att,
    got,
    total_ref,
    load_sem,
    asked_sem,
    w_send,
    w_recv,
    att_send,
    att_recv,
    need_send,
    need_recv,
    far_send,
    far_recv,
    lift_send,
    lift_recv,
    unit_send,
    unit_recv,
    sum_send,
    sum_recv,
    blk_send,
    blk_recv,
):
    kz, ky, kc, x = (lax.axis_index(name) for name in KV_TP)
    kp = ky * 2 + kc
    me = kz * PLANE + kp
    units = (unit_0, unit_1, unit_2)

    def in_plane(p):
        return (kz, p // 2, lax.rem(p, 2), x)

    def above(hops):
        return (lax.rem(kz + hops, N_Z), ky, kc, x)

    left, right, far = (lax.rem(x + hop, N_TP) for hop in (3, 1, 2))
    barrier = pltpu.get_barrier_semaphore()

    def signal(device):
        pl.semaphore_signal(barrier, inc=1, device_id=device, device_id_type=MESH)

    for peer in (left, right, far):
        signal((kz, ky, kc, peer))
    for hops in (1, 2, 3):
        signal(above(hops))
    for hop in range(1, PLANE):
        signal(in_plane(lax.rem(kp + hop, PLANE)))
    edge = jnp.logical_or(kz == 0, kz == N_Z - 1)

    def across(p):
        return (N_Z - 1 - kz, p // 2, lax.rem(p, 2), x)

    @pl.when(edge)
    def _():
        for hop in range(1, PLANE):
            signal(across(lax.rem(kp + hop, PLANE)))

    loads = []

    def load(src, dst):
        loads.append(pltpu.make_async_copy(src, dst, load_sem.at[len(loads)]))
        loads[-1].start()
        return loads[-1]

    steps = D // CHUNK
    kv_loads = []
    for k in range(steps):
        rows = pl.ds(k * CHUNK, CHUNK)
        kv_loads.append(
            (
                load(wk_hbm.at[rows], wkv.at[rows, pl.ds(0, 128)]),
                load(wv_hbm.at[rows], wkv.at[rows, pl.ds(128, 128)]),
                load(tok_hbm.at[:, rows], tok.at[:, rows]),
            )
        )
    wq_load = load(wq_hbm, wq)
    wg_load = load(wg_hbm, wg.at[pl.ds(0, 64)])
    wo_load = load(wo_hbm, wall.at[pl.ds(pl.multiple_of(x * WIDTH, WIDTH), WIDTH)])
    with jax.named_scope("barrier_wait"):
        peers_met = PLANE - 1 + N_Z - 1 + N_TP - 1
        pl.semaphore_wait(barrier, peers_met + jnp.where(edge, PLANE - 1, 0))

    def remote(src, dst, send, recv, device):
        return pltpu.make_async_remote_copy(
            src_ref=src,
            dst_ref=dst,
            send_sem=send,
            recv_sem=recv,
            device_id=device,
            device_id_type=MESH,
        )

    def need_copy(p, sender):
        return remote(
            need_ref.at[:, p], asked.at[sender], need_send.at[p], need_recv.at[sender], in_plane(p)
        )

    def peers(fn):
        def step(p, carry):
            @pl.when(p != kp)
            def _():
                fn(p)

            return carry

        lax.fori_loop(0, PLANE, step, 0)

    color = lax.rem(ky + kz, 2)
    mine_row = color * 256 + kc * 128
    other_row = (1 - color) * 256 + kc * 128

    def region(shard, row, count):
        return wall.at[pl.ds(pl.multiple_of(shard * WIDTH + row, 8), count)]

    def w_copy(index, src, dst, device):
        return remote(src, dst, w_send.at[index], w_recv.at[index], device)

    def w_first(side, piece, receiving=False):
        row = mine_row + 32 * piece
        shard = ((left, right)[side]) if receiving else x
        src = region(shard, row, 32)
        dst = src
        if not receiving:
            src = wo_hbm.at[pl.ds(pl.multiple_of(row, 32), 32)]
        return w_copy(4 * side + piece, src, dst, (kz, ky, kc, (right, left)[side]))

    def w_relay(piece, receiving=False):
        side = piece // 2
        part = region(far if receiving else (left, right)[side], mine_row + 32 * piece, 32)
        return w_copy(8 + piece, part, part, (kz, ky, kc, (right, left)[side]))

    directions = (
        (kz, lax.rem(ky + 1, 4), kc, x),
        (kz, lax.rem(ky + 3, 4), kc, x),
        (lax.rem(kz + 1, 4), ky, kc, x),
        (lax.rem(kz + 3, 4), ky, kc, x),
    )
    shards = (left, right, far)

    def w_second(o, piece, j, receiving=False):
        row = (other_row if receiving else mine_row) + 32 * piece + 8 * j
        part = region(shards[o], row, 8)
        return w_copy(12 + 16 * o + 4 * piece + j, part, part, directions[j])

    def w_third(half, o, piece, receiving=False):
        row = (mine_row, other_row)[half] + 32 * piece
        row = row - kc * 128 + (1 - kc) * 128 if receiving else row
        part = region(shards[o], row, 32)
        return w_copy(60 + 12 * half + 4 * o + piece, part, part, (kz, ky, 1 - kc, x))

    def w_spread(o, piece):
        for j in range(4):
            w_second(o, piece, j).start()
        w_third(0, o, piece).start()

    def w_swap(o):
        for piece in range(4):
            for j in range(4):
                w_second(o, piece, j, True).wait_recv()
            w_third(1, o, piece).start()

    for piece in range(4):
        w_first(0, piece).start()
        w_first(1, (piece + 2) % 4).start()

    with jax.named_scope("plan"):
        make_plan(me, chosen_ref, need_ref, index_ref, bias_ref)
        need_load = pltpu.make_async_copy(need_ref, need_s, load_sem.at[15])
        need_load.start()
        index_load = pltpu.make_async_copy(index_ref, index_s, load_sem.at[16])
        index_load.start()
    peers(lambda p: need_copy(p, kp).start())

    def need_far(p, sender):
        return remote(
            need_ref.at[0, p],
            asked_far.at[sender],
            far_send.at[p],
            far_recv.at[sender],
            across(p),
        )

    def everyone(fn):
        def step(p, carry):
            fn(p)
            return carry

        lax.fori_loop(0, PLANE, step, 0)

    @pl.when(kz == N_Z - 1)
    def _():
        everyone(lambda p: need_far(p, kp).start())

    wg[64:] = jnp.zeros((64, D), BF16)

    def clear(d, carry):
        sums[d // PLANE, lax.rem(d, PLANE)] = jnp.zeros(sums.shape[2:], BF16)
        return carry

    lax.fori_loop(me + 1, N_KV, clear, 0)

    with jax.named_scope("kv_proj"):
        for k in range(steps):
            for copy in kv_loads[k]:
                copy.wait()
            ks = slice(k * CHUNK, (k + 1) * CHUNK)
            for rows in HALVES:
                part = nn_dot(tok[rows, ks], wkv[ks])
                acc[rows, :256] = part if k == 0 else acc[rows, :256] + part
    low = lax.broadcasted_iota(jnp.int32, (ROWS, 128), 1) < HD
    keys = acc[:, :128].astype(BF16).astype(F32)
    values = acc[:, 128:256].astype(BF16).astype(F32)
    pairs = (
        jnp.where(low, keys, pltpu.roll(values, HD, 1)),
        jnp.where(low, pltpu.roll(keys, HD, 1), values),
    )
    offsets = pos_ref[...].astype(F32)
    offsets = jnp.concatenate([offsets, offsets], axis=1)
    lane_low = lax.broadcasted_iota(jnp.int32, (CMP, 128), 1) < HD
    row_head = lax.broadcasted_iota(jnp.int32, (8, CMP), 0)
    diagonal = lax.broadcasted_iota(jnp.int32, (CMP, CMP), 0) == lax.broadcasted_iota(
        jnp.int32, (CMP, CMP), 1
    )

    def column(ref, head):
        row = jnp.sum(jnp.where(row_head == head, ref[...].astype(F32), 0.0), axis=0, keepdims=True)
        return jnp.sum(jnp.where(diagonal, row, 0.0), axis=1, keepdims=True)

    with jax.named_scope("summary"):
        tails = []
        for g in range(GROUPS):
            pair = pairs[g]
            blocks = pair.astype(BF16).reshape(BLOCKS, SB, 128)
            unit_0[g] = blocks
            table[4 * N_KV + g * BLOCKS : 4 * N_KV + (g + 1) * BLOCKS] = blocks
            head = x * GROUPS + g
            mixing = jnp.where(lane_low, column(kmix_ref, head), column(vmix_ref, head))
            spans = jnp.sum((pair.reshape(SPANS, CMP, 128) + offsets[None]) * mixing[None], axis=1)
            sums[kz, kp, 16 * g : 16 * g + 16] = spans[:16].astype(BF16)
            tails.append(spans[16:])
        sums[kz, kp, 32:] = jnp.concatenate(tails, axis=0).astype(BF16)

    def lift_copy(hops, receiving=False):
        part = sums.at[kz - hops if receiving else kz, kp]
        return remote(part, part, lift_send.at[hops], lift_recv.at[hops], above(hops))

    def sum_copy(hops, p, sender):
        part = sums.at[kz - hops, sender]
        k = hops * PLANE
        return remote(part, part, sum_send.at[k + p], sum_recv.at[k + sender], in_plane(p))

    def spread(hops, fn):
        def step(p, carry):
            @pl.when(p > kp if hops == 0 else p != kp)
            def _():
                fn(p)

            return carry

        lax.fori_loop(0, PLANE, step, 0)

    def arriving(hops, fn):
        def step(p, carry):
            @pl.when(p < kp if hops == 0 else p != kp)
            def _():
                fn(p)

            return carry

        lax.fori_loop(0, PLANE, step, 0)

    for hops in (1, 2, 3):

        @pl.when(kz + hops < N_Z)
        def _():
            lift_copy(hops).start()

    spread(0, lambda p: sum_copy(0, p, kp).start())

    def unit_copy(hops):
        return remote(
            units[hops - 1], units[hops], unit_send.at[hops], unit_recv.at[hops], above(1)
        )

    sends_unit = {1: kz < 3, 2: jnp.logical_or(kz == 1, kz == 2)}

    @pl.when(sends_unit[1])
    def _():
        unit_copy(1).start()

    with jax.named_scope("need_wait"):

        def take_need(p):
            need_copy(kp, p).wait_recv()
            pltpu.make_async_copy(asked.at[p], asked_s.at[p], asked_sem.at[p]).start()

        peers(take_need)
        peers(lambda p: pltpu.make_async_copy(asked.at[p], asked_s.at[p], asked_sem.at[p]).wait())
        need_load.wait()
        index_load.wait()

        @pl.when(kz == 0)
        def _():
            def take(p):
                need_far(p, p).wait_recv()
                copy = pltpu.make_async_copy(asked_far.at[p], asked_far_s.at[p], asked_sem.at[p])
                copy.start()
                copy.wait()

            everyone(take)


    def blk_copy(hops, p, sender):
        dst = table.at[pl.ds(((kz - hops) * PLANE + sender) * 4, 4)]
        k = hops * PLANE
        return remote(
            stage.at[hops, p], dst, blk_send.at[k + p], blk_recv.at[k + sender], in_plane(p)
        )

    def serve(hops):
        @pl.when(kz >= hops)
        def _():
            if hops:
                unit_copy(hops).wait_recv()
            if hops == 1:

                @pl.when(sends_unit[2])
                def _():
                    unit_copy(2).start()

            def one(p):
                for slot in range(4):
                    block = asked_s[p, kz - hops, 0, slot]
                    stage[hops, p, slot] = units[hops][slot // 2, block]
                blk_copy(hops, p, kp).start()

            spread(hops, one)
            if hops:
                for slot in range(4):
                    block = need_s[kz - hops, kp, 0, slot]
                    place = ((kz - hops) * PLANE + kp) * 4 + slot
                    table[place] = units[hops][slot // 2, block]

    with jax.named_scope("sum_pass"):
        for hops in (1, 2, 3):

            @pl.when(kz >= hops)
            def _():
                lift_copy(hops, True).wait_recv()
                spread(hops, lambda p: sum_copy(hops, p, kp).start())

    def far_copy(p, sender):
        return remote(
            stage.at[3, p],
            table.at[pl.ds(sender * 4, 4)],
            blk_send.at[3 * PLANE + p],
            blk_recv.at[3 * PLANE + sender],
            across(p),
        )

    with jax.named_scope("serve_0"):
        serve(0)

        @pl.when(kz == 0)
        def _():
            def one(p):
                for slot in range(4):
                    stage[3, p, slot] = unit_0[slot // 2, asked_far_s[p, 0, slot]]
                far_copy(p, kp).start()

            everyone(one)

    with jax.named_scope("q_proj"):
        wq_load.wait()
        for k in range(steps):
            ks = slice(k * CHUNK, (k + 1) * CHUNK)
            part = nn_dot(tok[:, ks], wq[ks])
            acc[...] = part if k == 0 else acc[...] + part
        for h in range(GROUPS * GROUP):
            tile = acc[:, 128 * (h // 2) : 128 * (h // 2) + 128]
            if h % 2:
                tile = pltpu.roll(tile, HD, 1)
            tile = jnp.where(low, tile, 0.0).astype(BF16) * BF16(HD**-0.5)
            qp[:, h // GROUP, h % GROUP] = tile.reshape(BLOCKS, SB, 128)
    with jax.named_scope("gates"):
        wg_load.wait()
        for half, rows in enumerate(HALVES):
            own = pltpu.roll(nt_dot(tok[rows], wg[...]), lax.rem(128 - x * 16, 128), 1)
            part = slice(half * BLOCKS // 2, (half + 1) * BLOCKS // 2)
            gates[part] = jax.nn.sigmoid(own).reshape(BLOCKS // 2, SB, 128)

    with jax.named_scope("sum_wait"):
        for hops in range(N_Z):

            @pl.when(kz >= hops)
            def _():
                arriving(hops, lambda p: sum_copy(hops, kp, p).wait_recv())

    lane = lax.broadcasted_iota(jnp.int32, (SB, N_SPANS), 1)
    tail = lane - N_KV * 16
    span = jnp.where(
        tail < 0,
        (lane // 16) * SPANS + lax.rem(lane, 16),
        (tail // 4) * SPANS + 16 + lax.rem(tail, 4),
    )
    gap = span * CMP + CMP - 1 - lax.broadcasted_iota(jnp.int32, (SB, N_SPANS), 0)
    row_c = lax.rem(lax.broadcasted_iota(jnp.int32, (GROUP * SB, 1), 0), SB)

    def with_ones(pair):
        first = lax.broadcasted_iota(jnp.int32, pair.shape, 1) < HD
        return jnp.where(first, 1.0, pair.astype(F32)).astype(BF16)

    def gate_cols(b, g, branch):
        cols = [
            gates[b][:, 2 * (GROUP * g + r) + branch : 2 * (GROUP * g + r) + branch + 1]
            for r in range(GROUP)
        ]
        return jnp.concatenate(cols, axis=0)

    for g in range(GROUPS):
        tails = [
            sums[s // PLANE, s % PLANE, 32:].astype(F32)[4 * g : 4 * g + 4] for s in range(N_KV)
        ]
        head = sums[:, :, 16 * g : 16 * g + 16].reshape(N_KV * 16, 128)
        tails = jnp.concatenate(tails, axis=0).astype(BF16)
        span_keys[g, : N_KV * 16] = head
        span_keys[g, N_KV * 16 :] = tails
        span_values[g, : N_KV * 16] = with_ones(head)
        span_values[g, N_KV * 16 :] = with_ones(tails)

    def weigh(g, width, biased):
        for c in range(GROUP * SB // STRIP):
            rows = slice(c * STRIP, (c + 1) * STRIP)
            part = biased(score[g, rows, :width], c)
            most = jnp.max(part, axis=1, keepdims=True)
            prob[g, rows, :width] = jnp.exp(part - most).astype(BF16)

    def combine(g, width, table_rows):
        halves = [
            nn_dot(prob[g, h * 128 : (h + 1) * 128, :width], table_rows[...]) for h in range(2)
        ]
        mixed = jnp.concatenate(halves, axis=0)
        return mixed / pltpu.roll(mixed, HD, 1)

    def compressed(b, carry):
        start = me * ROWS + b * SB
        mask[...] = jnp.where(gap <= start, 0.0, LOW)
        for g in range(GROUPS):
            score[g, :, :N_SPANS] = nt_dot(qp[b, g].reshape(GROUP * SB, 128), span_keys[g])

        def biased(part, c):
            first = (c * STRIP) % SB
            return part + mask[first : first + STRIP]

        for g in range(GROUPS):
            weigh(g, N_SPANS, biased)
        for g in range(GROUPS):
            factor = jnp.where(row_c + start >= CMP - 1, gate_cols(b, g, 0), 0.0)
            comp[b, g] = combine(g, N_SPANS, span_values.at[g]) * factor

        @pl.when(b == 0)
        def _():
            with jax.named_scope("serve_1"):
                serve(1)

        @pl.when(b == 1)
        def _():
            with jax.named_scope("relay"):
                for piece in (0, 2, 1, 3):
                    w_first(piece // 2, piece, True).wait_recv()
                    w_relay(piece).start()

        @pl.when(b == BLOCKS - 1)
        def _():
            with jax.named_scope("serve_2"):
                serve(2)

        return carry

    with jax.named_scope("comp"):
        lax.fori_loop(0, BLOCKS, compressed, 0)

    with jax.named_scope("w1_wait"):
        for side in range(2):
            for piece in range(4):
                if piece // 2 != side:
                    w_first(side, piece, True).wait_recv()
                w_spread(side, piece)
    with jax.named_scope("blk_wait"):
        for hops in range(N_Z - 1):

            @pl.when(kz >= hops)
            def _():
                arriving(hops, lambda p: blk_copy(hops, kp, p).wait_recv())

        @pl.when(kz == N_Z - 1)
        def _():
            everyone(lambda p: far_copy(p, p).wait_recv())

    lane_first = lax.broadcasted_iota(jnp.int32, (STRIP, 128), 1)
    row_first = lax.broadcasted_iota(jnp.int32, (STRIP, 128), 0)
    low_half = lax.broadcasted_iota(jnp.int32, (SB, 128), 1) < HD

    def att_copy(target, sender):
        rows = pl.ds(pl.multiple_of(target * OUT_ROWS, 32), OUT_ROWS)
        return remote(
            att.at[rows],
            got.at[sender],
            att_send.at[target],
            att_recv.at[sender],
            (kz, ky, kc, target),
        )

    first_block = lax.rem(5 * (x + 1) // 2, BLOCKS)

    def chosen_block(i, carry):
        b = lax.rem(first_block + i, BLOCKS)
        for g in range(GROUPS):
            for s in range(N_SEL):
                piece = table[index_s[g, b, s]]
                keys_in[g, s * SB : (s + 1) * SB] = piece
                values_in[g, s * SB : (s + 1) * SB] = with_ones(piece)
            score[g] = nt_dot(qp[b, g].reshape(GROUP * SB, 128), keys_in[g])
        for g in range(GROUPS):

            def biased(part, c):
                part = part + bias_ref[g, b]
                seen = lane_first <= row_first + (c * STRIP) % SB
                seen = jnp.logical_or(lane_first >= SB, seen)
                return jnp.concatenate(
                    [jnp.where(seen, part[:, :128], LOW), part[:, 128:]], axis=1
                )

            weigh(g, N_SEL * SB, biased)
        for g in range(GROUPS):
            both = comp[b, g] + combine(g, N_SEL * SB, values_in.at[g]) * gate_cols(b, g, 1)
            for half in range(2):
                even = both[(2 * half) * SB : (2 * half + 1) * SB]
                odd = both[(2 * half + 1) * SB : (2 * half + 2) * SB]
                tile = jnp.where(low_half, pltpu.roll(even, HD, 1), odd).astype(BF16)
                lanes = slice(256 * g + 128 * half, 256 * g + 128 * half + 128)
                att[pl.ds(pl.multiple_of(b * SB, SB), SB), lanes] = tile
        for hop, last in ((1, 2), (2, 5), (3, 7)):

            @pl.when(i == last)
            def _():
                target = lax.rem(x + hop, N_TP)
                att_copy(target, x).start()

        for last, pieces in ((5, (0, 2)), (8, (1, 3))):

            @pl.when(i == last)
            def _():
                with jax.named_scope("w1_far"):
                    for piece in pieces:
                        w_relay(piece, True).wait_recv()
                        w_spread(2, piece)

        return carry

    with jax.named_scope("chosen"):
        lax.fori_loop(0, BLOCKS, chosen_block, 0)

    with jax.named_scope("w2_near"):
        w_swap(0)
        w_swap(1)
    with jax.named_scope("wo_wait"):
        wo_load.wait()
    got[x] = att[pl.ds(pl.multiple_of(x * OUT_ROWS, 32), OUT_ROWS)]
    for order, shard in enumerate((x, left, right, far)):
        if order:
            with jax.named_scope("w3_wait"):
                att_copy(shard, shard).wait_recv()
                for piece in range(4):
                    w_third(0, order - 1, piece, True).wait_recv()
                    w_third(1, order - 1, piece, True).wait_recv()

        def project(n, carry):
            cols = pl.ds(pl.multiple_of(n * CHUNK, CHUNK), CHUNK)
            rows = pl.ds(pl.multiple_of(shard * WIDTH, WIDTH), WIDTH)
            part = nn_dot(got[shard], wall[rows, cols])
            if order:
                part = part + total_ref[:, cols]
            if order < 3:
                total_ref[:, cols] = part
            else:
                out_ref[:, cols] = part.astype(BF16)
            return carry

        with jax.named_scope("outproj"):
            lax.fori_loop(0, D // CHUNK, project, 0)
        if order == 1:
            with jax.named_scope("w2_far"):
                w_swap(2)

    with jax.named_scope("drain"):
        peers(lambda p: need_copy(p, kp).wait_send())

        @pl.when(kz == N_Z - 1)
        def _():
            everyone(lambda p: need_far(p, kp).wait_send())

        @pl.when(kz == 0)
        def _():
            everyone(lambda p: far_copy(p, kp).wait_send())

        for piece in range(4):
            w_first(0, piece).wait_send()
            w_first(1, piece).wait_send()
            w_relay(piece).wait_send()
            for o in range(3):
                for j in range(4):
                    w_second(o, piece, j).wait_send()
                w_third(0, o, piece).wait_send()
                w_third(1, o, piece).wait_send()
        for hop in (1, 2, 3):
            att_copy(lax.rem(x + hop, N_TP), x).wait_send()
        for hops in (1, 2, 3):

            @pl.when(kz + hops < N_Z)
            def _():
                lift_copy(hops).wait_send()

        for hops in (1, 2):

            @pl.when(sends_unit[hops])
            def _():
                unit_copy(hops).wait_send()

        for hops in range(N_Z):

            @pl.when(kz >= hops)
            def _():
                def done(p):
                    sum_copy(hops, p, kp).wait_send()
                    if hops < 3:
                        blk_copy(hops, p, kp).wait_send()

                spread(hops, done)


def local(
    tokens,
    query_weight,
    key_weight,
    value_weight,
    gate_weight,
    summary_pos,
    key_mixing,
    value_mixing,
    out_weight,
    chosen,
):
    any_space = pl.BlockSpec(memory_space=pltpu.HBM)
    vmem = pl.BlockSpec(memory_space=pltpu.VMEM)
    dma = pltpu.SemaphoreType.DMA
    unit = pltpu.VMEM((GROUPS, BLOCKS, SB, 128), BF16)
    requests = (N_Z, PLANE, 1, 128)
    return pl.pallas_call(
        body,
        out_shape=pltpu.VMEM((OUT_ROWS, D), BF16),
        in_specs=[any_space] * 5 + [vmem] * 3 + [any_space, vmem],
        out_specs=vmem,
        scratch_shapes=[
            pltpu.VMEM((ROWS, D), BF16),
            pltpu.VMEM((D, WIDTH), BF16),
            pltpu.VMEM((D, 256), BF16),
            pltpu.VMEM((128, D), BF16),
            pltpu.VMEM((ROWS, WIDTH), F32),
            pltpu.VMEM((BLOCKS, SB, 128), F32),
            pltpu.VMEM((BLOCKS, GROUPS, GROUP, SB, 128), BF16),
            pltpu.VMEM((N_Z, PLANE, 40, 128), BF16),
            pltpu.VMEM((PLANE, N_Z, 1, 128), jnp.int32),
            pltpu.SMEM((PLANE, N_Z, 1, 128), jnp.int32),
            pltpu.VMEM((PLANE, 1, 128), jnp.int32),
            pltpu.SMEM((PLANE, 1, 128), jnp.int32),
            pltpu.VMEM((4 * N_KV + GROUPS * BLOCKS, SB, 128), BF16),
            pltpu.VMEM((N_Z, PLANE, 4, SB, 128), BF16),
            unit,
            unit,
            unit,
            pltpu.VMEM((BLOCKS, GROUPS, GROUP * SB, 128), F32),
            pltpu.VMEM((GROUPS, GROUP * SB, N_SEL * SB), F32),
            pltpu.VMEM((GROUPS, GROUP * SB, N_SEL * SB), BF16),
            pltpu.VMEM((GROUPS, N_SEL * SB, 128), BF16),
            pltpu.VMEM((GROUPS, N_SEL * SB, 128), BF16),
            pltpu.VMEM((GROUPS, N_SPANS, 128), BF16),
            pltpu.VMEM((GROUPS, N_SPANS, 128), BF16),
            pltpu.VMEM((SB, N_SPANS), F32),
            pltpu.VMEM(requests, jnp.int32),
            pltpu.SMEM(requests, jnp.int32),
            pltpu.VMEM((GROUPS, 16, 128), jnp.int32),
            pltpu.SMEM((GROUPS, 16, 128), jnp.int32),
            pltpu.VMEM((GROUPS, BLOCKS, 1, N_SEL * SB), F32),
            pltpu.VMEM((N_TP * WIDTH, D), BF16),
            pltpu.VMEM((ROWS, WIDTH), BF16),
            pltpu.VMEM((N_TP, OUT_ROWS, WIDTH), BF16),
            pltpu.VMEM((OUT_ROWS, D), F32),
            dma((17,)),
            dma((PLANE,)),
            dma((84,)),
            dma((84,)),
            dma((N_TP,)),
            dma((N_TP,)),
            dma((PLANE,)),
            dma((PLANE,)),
            dma((PLANE,)),
            dma((PLANE,)),
            dma((N_Z,)),
            dma((N_Z,)),
            dma((N_Z,)),
            dma((N_Z,)),
            dma((N_KV,)),
            dma((N_KV,)),
            dma((N_KV,)),
            dma((N_KV,)),
        ],
        compiler_params=pltpu.CompilerParams(
            collective_id=0, has_side_effects=True, vmem_limit_bytes=VMEM_MIB * 1024 * 1024
        ),
    )(
        tokens,
        query_weight,
        key_weight,
        value_weight,
        gate_weight.T,
        summary_pos,
        key_mixing.T,
        value_mixing.T,
        out_weight,
        chosen,
    )


def solution(mesh):
    torus = Mesh(mesh.devices.reshape(4, 4, 2, mesh.shape["tp"]), ("kv_0", "kv_1", "kv_2", "tp"))
    in_specs = (
        P(KV, None),
        P(None, "tp"),
        P(None, "tp"),
        P(None, "tp"),
        P(),
        P(),
        P(),
        P(),
        P("tp", None),
        P(KV, "tp", None),
    )
    out_specs = P(KV_TP, None)
    return jax.shard_map(local, mesh=torus, in_specs=in_specs, out_specs=out_specs, check_vma=False)
```

```python
import jax
import jax.numpy as jnp
from jax import lax
from jax.experimental import pallas as pl
from jax.experimental.pallas import tpu as pltpu
from jax.sharding import Mesh
from jax.sharding import PartitionSpec as P

HD = 64
CMP = 32
SB = 64
N_SEL = 16
N_KV = 32
N_Z = 4
PLANE = 8
N_TP = 4
ROWS = 640
BLOCKS = 10
GROUPS = 2
GROUP = 4
DIRECTIONS = ((0, 0, 8), (1, 8, 8), (2, 16, 8), (3, 24, 8))
SPANS = 20
N_SPANS = 640
VMEM_MIB = 58
STRIP = 32
HALVES = (slice(0, 320), slice(320, 640))
WIDTH = 512
OUT_ROWS = 160
D = 4096
CHUNK = 1024
KV = ("kv_0", "kv_1", "kv_2")
KV_TP = ("kv_0", "kv_1", "kv_2", "tp")
MESH = pl.DeviceIdType.MESH
BF16 = jnp.bfloat16
F32 = jnp.float32
LOW = -1e30


def nt_dot(a, b):
    return lax.dot_general(a, b, (((1,), (1,)), ((), ())), preferred_element_type=F32)


def nn_dot(a, b):
    return jnp.dot(a, b, preferred_element_type=F32)


def plan_requests(chosen_ref, need_ref):
    need_lane = lax.broadcasted_iota(jnp.int32, (1, 128), 1)
    named = [chosen_ref[:, g, :] for g in range(GROUPS)]
    sources = [n // BLOCKS for n in named]
    places = [n - s * BLOCKS for n, s in zip(named, sources)]
    firsts = [jnp.zeros((BLOCKS, N_SEL), jnp.int32) for _ in range(GROUPS)]
    for s in range(N_KV):
        ends = []
        for g in range(GROUPS):
            hit = sources[g] == s
            low = jnp.where(hit, BLOCKS - 1 - places[g], 0)
            high = jnp.where(hit, places[g], 0)
            ends += [jnp.max(v, axis=0, keepdims=True) for v in (low, high)]
        ends = jnp.max(jnp.concatenate(ends, axis=0), axis=1, keepdims=True)
        row = jnp.zeros((1, 128), jnp.int32)
        for g in range(GROUPS):
            first = BLOCKS - 1 - ends[2 * g : 2 * g + 1]
            firsts[g] = jnp.where(sources[g] == s, first, firsts[g])
            row = jnp.where(need_lane == 2 * g, first, row)
            row = jnp.where(need_lane == 2 * g + 1, ends[2 * g + 1 : 2 * g + 2], row)
        need_ref[s // PLANE, s % PLANE] = row
    return named, sources, places, firsts


def plan_blocks(me, plan, index_ref, bias_ref):
    named, sources, places, firsts = plan
    lane = lax.broadcasted_iota(jnp.int32, (BLOCKS, N_SEL), 1)
    spread = lax.broadcasted_iota(jnp.int32, (N_SEL, N_SEL * SB), 1) // SB
    spread = spread == lax.broadcasted_iota(jnp.int32, (N_SEL, N_SEL * SB), 0)
    spread = jnp.where(spread, 1.0, 0.0).astype(BF16)
    for g in range(GROUPS):
        repeated = jnp.zeros((BLOCKS, N_SEL), F32)
        for t in range(N_SEL - 1):
            same = jnp.logical_and(named[g] == named[g][:, t : t + 1], lane > t)
            repeated = jnp.where(same, 1.0, repeated)
        bias = nn_dot(repeated.astype(BF16), spread) * LOW
        for b in range(BLOCKS):
            bias_ref[g, b] = bias[b : b + 1]
        away = (sources[g] * GROUPS + g) * 2 + jnp.where(places[g] == firsts[g], 0, 1)
        home = 4 * N_KV + g * BLOCKS + places[g]
        index_ref[g, :BLOCKS, :N_SEL] = jnp.where(sources[g] == me, home, away)


def body(
    tok_hbm,
    wq_hbm,
    wk_hbm,
    wv_hbm,
    wg_hbm,
    pos_ref,
    kmix_ref,
    vmix_ref,
    wo_hbm,
    chosen_ref,
    out_ref,
    tok,
    wq,
    wkv,
    wg,
    acc,
    gates,
    qp,
    sums,
    asked,
    asked_s,
    asked_far,
    asked_far_s,
    table,
    stage,
    unit_0,
    unit_1,
    unit_2,
    comp,
    score,
    prob,
    keys_in,
    values_in,
    span_keys,
    span_values,
    mask,
    need_ref,
    need_s,
    index_ref,
    index_s,
    bias_ref,
    wall,
    att,
    got,
    total_ref,
    load_sem,
    asked_sem,
    w_send,
    w_recv,
    att_send,
    att_recv,
    need_send,
    need_recv,
    far_send,
    far_recv,
    lift_send,
    lift_recv,
    unit_send,
    unit_recv,
    sum_send,
    sum_recv,
    blk_send,
    blk_recv,
):
    kz, ky, kc, x = (lax.axis_index(name) for name in KV_TP)
    kp = ky * 2 + kc
    me = kz * PLANE + kp
    units = (unit_0, unit_1, unit_2)

    def in_plane(p):
        return (kz, p // 2, lax.rem(p, 2), x)

    def above(hops):
        return (lax.rem(kz + hops, N_Z), ky, kc, x)

    left, right, far = (lax.rem(x + hop, N_TP) for hop in (3, 1, 2))
    barrier = pltpu.get_barrier_semaphore()

    def signal(device):
        pl.semaphore_signal(barrier, inc=1, device_id=device, device_id_type=MESH)

    for peer in (left, right, far):
        signal((kz, ky, kc, peer))
    for hops in (1, 2, 3):
        signal(above(hops))
    for hop in range(1, PLANE):
        signal(in_plane(lax.rem(kp + hop, PLANE)))
    edge = jnp.logical_or(kz == 0, kz == N_Z - 1)

    def across(p):
        return (N_Z - 1 - kz, p // 2, lax.rem(p, 2), x)

    @pl.when(edge)
    def _():
        for hop in range(1, PLANE):
            signal(across(lax.rem(kp + hop, PLANE)))

    loads = []

    def load(src, dst):
        loads.append(pltpu.make_async_copy(src, dst, load_sem.at[len(loads)]))
        loads[-1].start()
        return loads[-1]

    steps = D // CHUNK
    kv_loads = []
    for k in range(steps):
        rows = pl.ds(k * CHUNK, CHUNK)
        kv_loads.append(
            (
                load(wk_hbm.at[rows], wkv.at[rows, pl.ds(0, 128)]),
                load(wv_hbm.at[rows], wkv.at[rows, pl.ds(128, 128)]),
                load(tok_hbm.at[:, rows], tok.at[:, rows]),
            )
        )
    wq_load = load(wq_hbm, wq)
    wg_load = load(wg_hbm, wg.at[pl.ds(0, 64)])
    wo_load = load(wo_hbm, wall.at[pl.ds(pl.multiple_of(x * WIDTH, WIDTH), WIDTH)])
    with jax.named_scope("barrier_wait"):
        peers_met = PLANE - 1 + N_Z - 1 + N_TP - 1
        pl.semaphore_wait(barrier, peers_met + jnp.where(edge, PLANE - 1, 0))

    def remote(src, dst, send, recv, device):
        return pltpu.make_async_remote_copy(
            src_ref=src,
            dst_ref=dst,
            send_sem=send,
            recv_sem=recv,
            device_id=device,
            device_id_type=MESH,
        )

    def need_copy(p, sender):
        return remote(
            need_ref.at[:, p], asked.at[sender], need_send.at[p], need_recv.at[sender], in_plane(p)
        )

    def peers(fn):
        def step(p, carry):
            @pl.when(p != kp)
            def _():
                fn(p)

            return carry

        lax.fori_loop(0, PLANE, step, 0)

    color = lax.rem(ky + kz, 2)
    mine_row = color * 256 + kc * 128
    other_row = (1 - color) * 256 + kc * 128

    def region(shard, row, count):
        return wall.at[pl.ds(pl.multiple_of(shard * WIDTH + row, 8), count)]

    def w_copy(index, src, dst, device):
        return remote(src, dst, w_send.at[index], w_recv.at[index], device)

    def w_first(side, piece, receiving=False):
        row = mine_row + 32 * piece
        shard = ((left, right)[side]) if receiving else x
        src = region(shard, row, 32)
        dst = src
        if not receiving:
            src = wo_hbm.at[pl.ds(pl.multiple_of(row, 32), 32)]
        return w_copy(4 * side + piece, src, dst, (kz, ky, kc, (right, left)[side]))

    def w_relay(piece, receiving=False):
        side = piece // 2
        part = region(far if receiving else (left, right)[side], mine_row + 32 * piece, 32)
        return w_copy(8 + piece, part, part, (kz, ky, kc, (right, left)[side]))

    directions = (
        (kz, lax.rem(ky + 1, 4), kc, x),
        (kz, lax.rem(ky + 3, 4), kc, x),
        (lax.rem(kz + 1, 4), ky, kc, x),
        (lax.rem(kz + 3, 4), ky, kc, x),
    )
    shards = (left, right, far)

    def slices(o, piece):
        return ((2, 0, 16), (3, 24, 8)) if piece // 2 == o else DIRECTIONS

    def w_second(o, piece, j, first, count, receiving=False, way=None):
        row = (other_row if receiving else mine_row) + 32 * piece + first
        part = region(shards[o], row, count)
        device = directions[j if way is None else way]
        return w_copy(12 + 16 * o + 4 * piece + j, part, part, device)

    def w_swing(o, piece, fn, receiving=False):
        if piece // 2 == o:
            last = kz == N_Z - 1

            @pl.when(jnp.logical_not(last) if receiving else kz != 0)
            def _():
                fn(w_second(o, piece, 1, 16, 8, receiving, 3))

            @pl.when(last if receiving else kz == N_Z - 2)
            def _():
                fn(w_second(o, piece, 0, 16, 8, receiving, 2))

    def w_third(half, o, piece, receiving=False):
        row = (mine_row, other_row)[half] + 32 * piece
        row = row - kc * 128 + (1 - kc) * 128 if receiving else row
        part = region(shards[o], row, 32)
        return w_copy(60 + 12 * half + 4 * o + piece, part, part, (kz, ky, 1 - kc, x))

    def w_spread(o, piece):
        for cut in slices(o, piece):
            w_second(o, piece, *cut).start()
        w_swing(o, piece, lambda copy: copy.start())
        w_third(0, o, piece).start()

    def w_swap(o, pieces):
        for piece in pieces:
            for cut in slices(o, piece):
                w_second(o, piece, *cut, True).wait_recv()
            w_swing(o, piece, lambda copy: copy.wait_recv(), True)
            w_third(1, o, piece).start()

    for piece in range(4):
        w_first(0, piece).start()
        w_first(1, (piece + 2) % 4).start()

    with jax.named_scope("plan"):
        plan = plan_requests(chosen_ref, need_ref)
        need_load = pltpu.make_async_copy(need_ref, need_s, load_sem.at[15])
        need_load.start()
    peers(lambda p: need_copy(p, kp).start())

    def need_far(p, sender):
        return remote(
            need_ref.at[0, p],
            asked_far.at[sender],
            far_send.at[p],
            far_recv.at[sender],
            across(p),
        )

    def everyone(fn):
        def step(p, carry):
            fn(p)
            return carry

        lax.fori_loop(0, PLANE, step, 0)

    @pl.when(kz == N_Z - 1)
    def _():
        everyone(lambda p: need_far(p, kp).start())

    wg[64:] = jnp.zeros((64, D), BF16)

    def clear(d, carry):
        sums[d // PLANE, lax.rem(d, PLANE)] = jnp.zeros(sums.shape[2:], BF16)
        return carry

    lax.fori_loop(me + 1, N_KV, clear, 0)

    with jax.named_scope("kv_proj"):
        for k in range(steps):
            for copy in kv_loads[k]:
                copy.wait()
            ks = slice(k * CHUNK, (k + 1) * CHUNK)
            for rows in HALVES:
                part = nn_dot(tok[rows, ks], wkv[ks])
                acc[rows, :256] = part if k == 0 else acc[rows, :256] + part
    low = lax.broadcasted_iota(jnp.int32, (ROWS, 128), 1) < HD
    keys = acc[:, :128].astype(BF16).astype(F32)
    values = acc[:, 128:256].astype(BF16).astype(F32)
    pairs = (
        jnp.where(low, keys, pltpu.roll(values, HD, 1)),
        jnp.where(low, pltpu.roll(keys, HD, 1), values),
    )
    offsets = pos_ref[...].astype(F32)
    offsets = jnp.concatenate([offsets, offsets], axis=1)
    lane_low = lax.broadcasted_iota(jnp.int32, (CMP, 128), 1) < HD
    row_head = lax.broadcasted_iota(jnp.int32, (8, CMP), 0)
    diagonal = lax.broadcasted_iota(jnp.int32, (CMP, CMP), 0) == lax.broadcasted_iota(
        jnp.int32, (CMP, CMP), 1
    )

    def column(ref, head):
        row = jnp.sum(jnp.where(row_head == head, ref[...].astype(F32), 0.0), axis=0, keepdims=True)
        return jnp.sum(jnp.where(diagonal, row, 0.0), axis=1, keepdims=True)

    with jax.named_scope("summary"):
        tails = []
        for g in range(GROUPS):
            pair = pairs[g]
            blocks = pair.astype(BF16).reshape(BLOCKS, SB, 128)
            unit_0[g] = blocks
            table[4 * N_KV + g * BLOCKS : 4 * N_KV + (g + 1) * BLOCKS] = blocks
            head = x * GROUPS + g
            mixing = jnp.where(lane_low, column(kmix_ref, head), column(vmix_ref, head))
            spans = jnp.sum((pair.reshape(SPANS, CMP, 128) + offsets[None]) * mixing[None], axis=1)
            sums[kz, kp, 16 * g : 16 * g + 16] = spans[:16].astype(BF16)
            tails.append(spans[16:])
        sums[kz, kp, 32:] = jnp.concatenate(tails, axis=0).astype(BF16)

    def lift_copy(hops, receiving=False):
        part = sums.at[kz - hops if receiving else kz, kp]
        return remote(part, part, lift_send.at[hops], lift_recv.at[hops], above(hops))

    def sum_copy(hops, p, sender):
        part = sums.at[kz - hops, sender]
        k = hops * PLANE
        return remote(part, part, sum_send.at[k + p], sum_recv.at[k + sender], in_plane(p))

    def spread(hops, fn):
        def step(p, carry):
            @pl.when(p > kp if hops == 0 else p != kp)
            def _():
                fn(p)

            return carry

        lax.fori_loop(0, PLANE, step, 0)

    def arriving(hops, fn):
        def step(p, carry):
            @pl.when(p < kp if hops == 0 else p != kp)
            def _():
                fn(p)

            return carry

        lax.fori_loop(0, PLANE, step, 0)

    for hops in (1, 2, 3):

        @pl.when(kz + hops < N_Z)
        def _():
            lift_copy(hops).start()

    spread(0, lambda p: sum_copy(0, p, kp).start())

    def unit_copy(hops, g):
        src, dst, k = units[hops - 1].at[g], units[hops].at[g], hops * GROUPS + g
        return remote(src, dst, unit_send.at[k], unit_recv.at[k], above(1))

    sends_unit = {1: kz < 3, 2: jnp.logical_or(kz == 1, kz == 2)}

    @pl.when(sends_unit[1])
    def _():
        for g in range(GROUPS):
            unit_copy(1, g).start()

    with jax.named_scope("gates"):
        wg_load.wait()
        for half, rows in enumerate(HALVES):
            own = pltpu.roll(nt_dot(tok[rows], wg[...]), lax.rem(128 - x * 16, 128), 1)
            part = slice(half * BLOCKS // 2, (half + 1) * BLOCKS // 2)
            gates[part] = jax.nn.sigmoid(own).reshape(BLOCKS // 2, SB, 128)

    with jax.named_scope("plan_blocks"):
        plan_blocks(me, plan, index_ref, bias_ref)
        index_load = pltpu.make_async_copy(index_ref, index_s, load_sem.at[16])
        index_load.start()
    with jax.named_scope("need_wait"):

        def take_need(p):
            need_copy(kp, p).wait_recv()
            pltpu.make_async_copy(asked.at[p], asked_s.at[p], asked_sem.at[p]).start()

        peers(take_need)
        peers(lambda p: pltpu.make_async_copy(asked.at[p], asked_s.at[p], asked_sem.at[p]).wait())
        need_load.wait()
        index_load.wait()

        @pl.when(kz == 0)
        def _():
            def take(p):
                need_far(p, p).wait_recv()
                copy = pltpu.make_async_copy(asked_far.at[p], asked_far_s.at[p], asked_sem.at[p])
                copy.start()
                copy.wait()

            everyone(take)


    def blk_copy(hops, p, sender):
        dst = table.at[pl.ds(((kz - hops) * PLANE + sender) * 4, 4)]
        k = hops * PLANE
        return remote(
            stage.at[hops, p], dst, blk_send.at[k + p], blk_recv.at[k + sender], in_plane(p)
        )

    def unit_pass(g):
        unit_copy(1, g).wait_recv()

        @pl.when(sends_unit[2])
        def _():
            unit_copy(2, g).start()

    def serve(hops):
        @pl.when(kz >= hops)
        def _():
            if hops == 1:
                unit_pass(1)
            if hops == 2:
                for g in range(GROUPS):
                    unit_copy(2, g).wait_recv()

            def one(p):
                for slot in range(4):
                    block = asked_s[p, kz - hops, 0, slot]
                    stage[hops, p, slot] = units[hops][slot // 2, block]
                blk_copy(hops, p, kp).start()

            spread(hops, one)
            if hops:
                for slot in range(4):
                    block = need_s[kz - hops, kp, 0, slot]
                    place = ((kz - hops) * PLANE + kp) * 4 + slot
                    table[place] = units[hops][slot // 2, block]

    with jax.named_scope("sum_pass"):
        for hops in (1, 2, 3):

            @pl.when(kz >= hops)
            def _():
                lift_copy(hops, True).wait_recv()
                spread(hops, lambda p: sum_copy(hops, p, kp).start())

    def far_copy(p, sender):
        return remote(
            stage.at[3, p],
            table.at[pl.ds(sender * 4, 4)],
            blk_send.at[3 * PLANE + p],
            blk_recv.at[3 * PLANE + sender],
            across(p),
        )

    with jax.named_scope("serve_0"):
        serve(0)

        @pl.when(kz == 0)
        def _():
            def one(p):
                for slot in range(4):
                    stage[3, p, slot] = unit_0[slot // 2, asked_far_s[p, 0, slot]]
                far_copy(p, kp).start()

            everyone(one)

    with jax.named_scope("q_proj"):
        wq_load.wait()
        for k in range(steps):
            ks = slice(k * CHUNK, (k + 1) * CHUNK)
            part = nn_dot(tok[:, ks], wq[ks])
            acc[...] = part if k == 0 else acc[...] + part
        for h in range(GROUPS * GROUP):
            tile = acc[:, 128 * (h // 2) : 128 * (h // 2) + 128]
            if h % 2:
                tile = pltpu.roll(tile, HD, 1)
            tile = jnp.where(low, tile, 0.0).astype(BF16) * BF16(HD**-0.5)
            qp[:, h // GROUP, h % GROUP] = tile.reshape(BLOCKS, SB, 128)
    with jax.named_scope("relay"):
        for piece in (0, 2):
            w_first(piece // 2, piece, True).wait_recv()
            w_relay(piece).start()

        @pl.when(kz >= 1)
        def _():
            unit_pass(0)

    with jax.named_scope("sum_wait"):
        for hops in range(N_Z):

            @pl.when(kz >= hops)
            def _():
                arriving(hops, lambda p: sum_copy(hops, kp, p).wait_recv())

    lane = lax.broadcasted_iota(jnp.int32, (SB, N_SPANS), 1)
    tail = lane - N_KV * 16
    span = jnp.where(
        tail < 0,
        (lane // 16) * SPANS + lax.rem(lane, 16),
        (tail // 4) * SPANS + 16 + lax.rem(tail, 4),
    )
    gap = span * CMP + CMP - 1 - lax.broadcasted_iota(jnp.int32, (SB, N_SPANS), 0)
    row_c = lax.rem(lax.broadcasted_iota(jnp.int32, (GROUP * SB, 1), 0), SB)

    def with_ones(pair):
        first = lax.broadcasted_iota(jnp.int32, pair.shape, 1) < HD
        return jnp.where(first, 1.0, pair.astype(F32)).astype(BF16)

    def gate_cols(b, g, branch):
        cols = [
            gates[b][:, 2 * (GROUP * g + r) + branch : 2 * (GROUP * g + r) + branch + 1]
            for r in range(GROUP)
        ]
        return jnp.concatenate(cols, axis=0)

    for g in range(GROUPS):
        tails = [
            sums[s // PLANE, s % PLANE, 32:].astype(F32)[4 * g : 4 * g + 4] for s in range(N_KV)
        ]
        head = sums[:, :, 16 * g : 16 * g + 16].reshape(N_KV * 16, 128)
        tails = jnp.concatenate(tails, axis=0).astype(BF16)
        span_keys[g, : N_KV * 16] = head
        span_keys[g, N_KV * 16 :] = tails
        span_values[g, : N_KV * 16] = with_ones(head)
        span_values[g, N_KV * 16 :] = with_ones(tails)

    def weigh(g, width, biased):
        for c in range(GROUP * SB // STRIP):
            rows = slice(c * STRIP, (c + 1) * STRIP)
            part = biased(score[g, rows, :width], c)
            most = jnp.max(part, axis=1, keepdims=True)
            prob[g, rows, :width] = jnp.exp(part - most).astype(BF16)

    def combine(g, width, table_rows):
        halves = [
            nn_dot(prob[g, h * 128 : (h + 1) * 128, :width], table_rows[...]) for h in range(2)
        ]
        mixed = jnp.concatenate(halves, axis=0)
        return mixed / pltpu.roll(mixed, HD, 1)

    def compressed(b, carry):
        start = me * ROWS + b * SB
        mask[...] = jnp.where(gap <= start, 0.0, LOW)
        for g in range(GROUPS):
            score[g, :, :N_SPANS] = nt_dot(qp[b, g].reshape(GROUP * SB, 128), span_keys[g])

        def biased(part, c):
            first = (c * STRIP) % SB
            return part + mask[first : first + STRIP]

        for g in range(GROUPS):
            weigh(g, N_SPANS, biased)
        for g in range(GROUPS):
            factor = jnp.where(row_c + start >= CMP - 1, gate_cols(b, g, 0), 0.0)
            comp[b, g] = combine(g, N_SPANS, span_values.at[g]) * factor

        @pl.when(b == 0)
        def _():
            with jax.named_scope("serve_1"):
                serve(1)

        @pl.when(b == 1)
        def _():
            with jax.named_scope("relay"):
                for piece in (1, 3):
                    w_first(piece // 2, piece, True).wait_recv()
                    w_relay(piece).start()

        @pl.when(b == 4)
        def _():
            for side in range(2):
                for piece in (2 * side, 2 * side + 1):
                    w_spread(side, piece)

        @pl.when(b == 6)
        def _():
            with jax.named_scope("serve_2"):
                serve(2)

        return carry

    with jax.named_scope("comp"):
        lax.fori_loop(0, BLOCKS, compressed, 0)

    with jax.named_scope("blk_wait"):
        for hops in range(N_Z - 1):

            @pl.when(kz >= hops)
            def _():
                arriving(hops, lambda p: blk_copy(hops, kp, p).wait_recv())

        @pl.when(kz == N_Z - 1)
        def _():
            everyone(lambda p: far_copy(p, p).wait_recv())

    lane_first = lax.broadcasted_iota(jnp.int32, (STRIP, 128), 1)
    row_first = lax.broadcasted_iota(jnp.int32, (STRIP, 128), 0)
    low_half = lax.broadcasted_iota(jnp.int32, (SB, 128), 1) < HD

    def att_copy(target, sender):
        rows = pl.ds(pl.multiple_of(target * OUT_ROWS, 32), OUT_ROWS)
        return remote(
            att.at[rows],
            got.at[sender],
            att_send.at[target],
            att_recv.at[sender],
            (kz, ky, kc, target),
        )

    first_block = lax.rem(5 * (x + 1) // 2, BLOCKS)

    def pass_far(pieces):
        for piece in pieces:
            w_relay(piece, True).wait_recv()
            w_spread(2, piece)

    def chosen_block(i, carry):
        b = lax.rem(first_block + i, BLOCKS)
        for g in range(GROUPS):
            for s in range(N_SEL):
                piece = table[index_s[g, b, s]]
                keys_in[g, s * SB : (s + 1) * SB] = piece
                values_in[g, s * SB : (s + 1) * SB] = with_ones(piece)
            score[g] = nt_dot(qp[b, g].reshape(GROUP * SB, 128), keys_in[g])
        for g in range(GROUPS):

            def biased(part, c):
                part = part + bias_ref[g, b]
                seen = lane_first <= row_first + (c * STRIP) % SB
                seen = jnp.logical_or(lane_first >= SB, seen)
                return jnp.concatenate(
                    [jnp.where(seen, part[:, :128], LOW), part[:, 128:]], axis=1
                )

            weigh(g, N_SEL * SB, biased)
        for g in range(GROUPS):
            both = comp[b, g] + combine(g, N_SEL * SB, values_in.at[g]) * gate_cols(b, g, 1)
            for half in range(2):
                even = both[(2 * half) * SB : (2 * half + 1) * SB]
                odd = both[(2 * half + 1) * SB : (2 * half + 2) * SB]
                tile = jnp.where(low_half, pltpu.roll(even, HD, 1), odd).astype(BF16)
                lanes = slice(256 * g + 128 * half, 256 * g + 128 * half + 128)
                att[pl.ds(pl.multiple_of(b * SB, SB), SB), lanes] = tile
        for hop, last in ((1, 2), (2, 5), (3, 7)):

            @pl.when(i == last)
            def _():
                target = lax.rem(x + hop, N_TP)
                att_copy(target, x).start()

        @pl.when(i == 1)
        def _():
            with jax.named_scope("w1_near"):
                for side in range(2):
                    for piece in (2 - 2 * side, 3 - 2 * side):
                        w_first(side, piece, True).wait_recv()
                        w_spread(side, piece)

        @pl.when(i == BLOCKS - 1)
        def _():
            with jax.named_scope("w2_early"):
                for side in range(2):
                    w_swap(side, (2 * side, 2 * side + 1))

        @pl.when(i == jnp.where(kz == 0, 5, 4))
        def _():
            with jax.named_scope("w1_far"):
                pass_far((0, 2))

        @pl.when(jnp.logical_and(i == 7, kz != 0))
        def _():
            with jax.named_scope("w1_far"):
                pass_far((1, 3))

        return carry

    with jax.named_scope("chosen"):
        lax.fori_loop(0, BLOCKS, chosen_block, 0)

    @pl.when(kz == 0)
    def _():
        with jax.named_scope("w1_far"):
            pass_far((1, 3))


    with jax.named_scope("w2_near"):
        w_swap(0, (2, 3))
        w_swap(1, (0, 1))
    with jax.named_scope("wo_wait"):
        wo_load.wait()
    got[x] = att[pl.ds(pl.multiple_of(x * OUT_ROWS, 32), OUT_ROWS)]
    for order, shard in enumerate((x, left, right, far)):
        if order:
            with jax.named_scope("w3_wait"):
                att_copy(shard, shard).wait_recv()
                for piece in range(4):
                    w_third(0, order - 1, piece, True).wait_recv()
                    w_third(1, order - 1, piece, True).wait_recv()

        def project(n, carry):
            cols = pl.ds(pl.multiple_of(n * CHUNK, CHUNK), CHUNK)
            rows = pl.ds(pl.multiple_of(shard * WIDTH, WIDTH), WIDTH)
            part = nn_dot(got[shard], wall[rows, cols])
            if order:
                part = part + total_ref[:, cols]
            if order < 3:
                total_ref[:, cols] = part
            else:
                out_ref[:, cols] = part.astype(BF16)
            return carry

        with jax.named_scope("outproj"):
            lax.fori_loop(0, D // CHUNK, project, 0)
        if order == 1:
            with jax.named_scope("w2_far"):
                w_swap(2, range(4))

    with jax.named_scope("drain"):
        peers(lambda p: need_copy(p, kp).wait_send())

        @pl.when(kz == N_Z - 1)
        def _():
            everyone(lambda p: need_far(p, kp).wait_send())

        @pl.when(kz == 0)
        def _():
            everyone(lambda p: far_copy(p, kp).wait_send())

        for piece in range(4):
            w_first(0, piece).wait_send()
            w_first(1, piece).wait_send()
            w_relay(piece).wait_send()
            for o in range(3):
                for cut in slices(o, piece):
                    w_second(o, piece, *cut).wait_send()
                w_swing(o, piece, lambda copy: copy.wait_send())
                w_third(0, o, piece).wait_send()
                w_third(1, o, piece).wait_send()
        for hop in (1, 2, 3):
            att_copy(lax.rem(x + hop, N_TP), x).wait_send()
        for hops in (1, 2, 3):

            @pl.when(kz + hops < N_Z)
            def _():
                lift_copy(hops).wait_send()

        for hops in (1, 2):

            @pl.when(sends_unit[hops])
            def _():
                for g in range(GROUPS):
                    unit_copy(hops, g).wait_send()

        for hops in range(N_Z):

            @pl.when(kz >= hops)
            def _():
                def done(p):
                    sum_copy(hops, p, kp).wait_send()
                    if hops < 3:
                        blk_copy(hops, p, kp).wait_send()

                spread(hops, done)


def local(
    tokens,
    query_weight,
    key_weight,
    value_weight,
    gate_weight,
    summary_pos,
    key_mixing,
    value_mixing,
    out_weight,
    chosen,
):
    any_space = pl.BlockSpec(memory_space=pltpu.HBM)
    vmem = pl.BlockSpec(memory_space=pltpu.VMEM)
    dma = pltpu.SemaphoreType.DMA
    unit = pltpu.VMEM((GROUPS, BLOCKS, SB, 128), BF16)
    requests = (N_Z, PLANE, 1, 128)
    return pl.pallas_call(
        body,
        out_shape=pltpu.VMEM((OUT_ROWS, D), BF16),
        in_specs=[any_space] * 5 + [vmem] * 3 + [any_space, vmem],
        out_specs=vmem,
        scratch_shapes=[
            pltpu.VMEM((ROWS, D), BF16),
            pltpu.VMEM((D, WIDTH), BF16),
            pltpu.VMEM((D, 256), BF16),
            pltpu.VMEM((128, D), BF16),
            pltpu.VMEM((ROWS, WIDTH), F32),
            pltpu.VMEM((BLOCKS, SB, 128), F32),
            pltpu.VMEM((BLOCKS, GROUPS, GROUP, SB, 128), BF16),
            pltpu.VMEM((N_Z, PLANE, 40, 128), BF16),
            pltpu.VMEM((PLANE, N_Z, 1, 128), jnp.int32),
            pltpu.SMEM((PLANE, N_Z, 1, 128), jnp.int32),
            pltpu.VMEM((PLANE, 1, 128), jnp.int32),
            pltpu.SMEM((PLANE, 1, 128), jnp.int32),
            pltpu.VMEM((4 * N_KV + GROUPS * BLOCKS, SB, 128), BF16),
            pltpu.VMEM((N_Z, PLANE, 4, SB, 128), BF16),
            unit,
            unit,
            unit,
            pltpu.VMEM((BLOCKS, GROUPS, GROUP * SB, 128), F32),
            pltpu.VMEM((GROUPS, GROUP * SB, N_SEL * SB), F32),
            pltpu.VMEM((GROUPS, GROUP * SB, N_SEL * SB), BF16),
            pltpu.VMEM((GROUPS, N_SEL * SB, 128), BF16),
            pltpu.VMEM((GROUPS, N_SEL * SB, 128), BF16),
            pltpu.VMEM((GROUPS, N_SPANS, 128), BF16),
            pltpu.VMEM((GROUPS, N_SPANS, 128), BF16),
            pltpu.VMEM((SB, N_SPANS), F32),
            pltpu.VMEM(requests, jnp.int32),
            pltpu.SMEM(requests, jnp.int32),
            pltpu.VMEM((GROUPS, 16, 128), jnp.int32),
            pltpu.SMEM((GROUPS, 16, 128), jnp.int32),
            pltpu.VMEM((GROUPS, BLOCKS, 1, N_SEL * SB), F32),
            pltpu.VMEM((N_TP * WIDTH, D), BF16),
            pltpu.VMEM((ROWS, WIDTH), BF16),
            pltpu.VMEM((N_TP, OUT_ROWS, WIDTH), BF16),
            pltpu.VMEM((OUT_ROWS, D), F32),
            dma((17,)),
            dma((PLANE,)),
            dma((84,)),
            dma((84,)),
            dma((N_TP,)),
            dma((N_TP,)),
            dma((PLANE,)),
            dma((PLANE,)),
            dma((PLANE,)),
            dma((PLANE,)),
            dma((N_Z,)),
            dma((N_Z,)),
            dma((N_Z * GROUPS,)),
            dma((N_Z * GROUPS,)),
            dma((N_KV,)),
            dma((N_KV,)),
            dma((N_KV,)),
            dma((N_KV,)),
        ],
        compiler_params=pltpu.CompilerParams(
            collective_id=0, has_side_effects=True, vmem_limit_bytes=VMEM_MIB * 1024 * 1024
        ),
    )(
        tokens,
        query_weight,
        key_weight,
        value_weight,
        gate_weight.T,
        summary_pos,
        key_mixing.T,
        value_mixing.T,
        out_weight,
        chosen,
    )


def solution(mesh):
    torus = Mesh(mesh.devices.reshape(4, 4, 2, mesh.shape["tp"]), ("kv_0", "kv_1", "kv_2", "tp"))
    in_specs = (
        P(KV, None),
        P(None, "tp"),
        P(None, "tp"),
        P(None, "tp"),
        P(),
        P(),
        P(),
        P(),
        P("tp", None),
        P(KV, "tp", None),
    )
    out_specs = P(KV_TP, None)
    return jax.shard_map(local, mesh=torus, in_specs=in_specs, out_specs=out_specs, check_vma=False)
```

```python
import jax
import jax.numpy as jnp
from jax import lax
from jax.experimental import pallas as pl
from jax.experimental.pallas import tpu as pltpu
from jax.sharding import Mesh
from jax.sharding import PartitionSpec as P

HD = 64
CMP = 32
SB = 64
N_SEL = 16
N_KV = 32
N_Z = 4
PLANE = 8
N_TP = 4
ROWS = 640
BLOCKS = 10
GROUPS = 2
GROUP = 4
DIRECTIONS = ((0, 0, 8), (1, 8, 8), (2, 16, 8), (3, 24, 8))
SPANS = 20
N_SPANS = 640
VMEM_MIB = 58
STRIP = 32
HALVES = (slice(0, 320), slice(320, 640))
WIDTH = 512
OUT_ROWS = 160
D = 4096
CHUNK = 1024
KV = ("kv_0", "kv_1", "kv_2")
KV_TP = ("kv_0", "kv_1", "kv_2", "tp")
MESH = pl.DeviceIdType.MESH
BF16 = jnp.bfloat16
F32 = jnp.float32
LOW = -1e30


def nt_dot(a, b):
    return lax.dot_general(a, b, (((1,), (1,)), ((), ())), preferred_element_type=F32)


def nn_dot(a, b):
    return jnp.dot(a, b, preferred_element_type=F32)


def plan_requests(chosen_ref, need_ref):
    need_lane = lax.broadcasted_iota(jnp.int32, (1, 128), 1)
    named = [chosen_ref[:, g, :] for g in range(GROUPS)]
    sources = [n // BLOCKS for n in named]
    places = [n - s * BLOCKS for n, s in zip(named, sources)]
    firsts = [jnp.zeros((BLOCKS, N_SEL), jnp.int32) for _ in range(GROUPS)]
    for s in range(N_KV):
        ends = []
        for g in range(GROUPS):
            hit = sources[g] == s
            low = jnp.where(hit, BLOCKS - 1 - places[g], 0)
            high = jnp.where(hit, places[g], 0)
            ends += [jnp.max(v, axis=0, keepdims=True) for v in (low, high)]
        ends = jnp.max(jnp.concatenate(ends, axis=0), axis=1, keepdims=True)
        row = jnp.zeros((1, 128), jnp.int32)
        for g in range(GROUPS):
            first = BLOCKS - 1 - ends[2 * g : 2 * g + 1]
            firsts[g] = jnp.where(sources[g] == s, first, firsts[g])
            row = jnp.where(need_lane == 2 * g, first, row)
            row = jnp.where(need_lane == 2 * g + 1, ends[2 * g + 1 : 2 * g + 2], row)
        need_ref[s // PLANE, s % PLANE] = row
    return named, sources, places, firsts


def plan_blocks(me, plan, index_ref, bias_ref):
    named, sources, places, firsts = plan
    lane = lax.broadcasted_iota(jnp.int32, (BLOCKS, N_SEL), 1)
    spread = lax.broadcasted_iota(jnp.int32, (N_SEL, N_SEL * SB), 1) // SB
    spread = spread == lax.broadcasted_iota(jnp.int32, (N_SEL, N_SEL * SB), 0)
    spread = jnp.where(spread, 1.0, 0.0).astype(BF16)
    for g in range(GROUPS):
        repeated = jnp.zeros((BLOCKS, N_SEL), F32)
        for t in range(N_SEL - 1):
            same = jnp.logical_and(named[g] == named[g][:, t : t + 1], lane > t)
            repeated = jnp.where(same, 1.0, repeated)
        bias = nn_dot(repeated.astype(BF16), spread) * LOW
        for b in range(BLOCKS):
            bias_ref[g, b] = bias[b : b + 1]
        away = (sources[g] * GROUPS + g) * 2 + jnp.where(places[g] == firsts[g], 0, 1)
        home = 4 * N_KV + g * BLOCKS + places[g]
        index_ref[g, :BLOCKS, :N_SEL] = jnp.where(sources[g] == me, home, away)


def body(
    tok_hbm,
    wq_hbm,
    wk_hbm,
    wv_hbm,
    wg_hbm,
    pos_ref,
    kmix_ref,
    vmix_ref,
    wo_hbm,
    chosen_ref,
    out_ref,
    tok,
    wq,
    wkv,
    wg,
    acc,
    gates,
    qp,
    sums,
    asked,
    asked_s,
    asked_far,
    asked_far_s,
    table,
    stage,
    unit_0,
    unit_1,
    unit_2,
    comp,
    score,
    prob,
    keys_in,
    values_in,
    span_keys,
    span_values,
    mask,
    need_ref,
    need_s,
    index_ref,
    index_s,
    bias_ref,
    wall,
    att,
    got,
    total_ref,
    load_sem,
    asked_sem,
    w_send,
    w_recv,
    att_send,
    att_recv,
    need_send,
    need_recv,
    far_send,
    far_recv,
    lift_send,
    lift_recv,
    unit_send,
    unit_recv,
    sum_send,
    sum_recv,
    blk_send,
    blk_recv,
):
    kz, ky, kc, x = (lax.axis_index(name) for name in KV_TP)
    kp = ky * 2 + kc
    me = kz * PLANE + kp
    units = (unit_0, unit_1, unit_2)

    def in_plane(p):
        return (kz, p // 2, lax.rem(p, 2), x)

    def above(hops):
        return (lax.rem(kz + hops, N_Z), ky, kc, x)

    left, right, far = (lax.rem(x + hop, N_TP) for hop in (3, 1, 2))
    barrier = pltpu.get_barrier_semaphore()

    def signal(device):
        pl.semaphore_signal(barrier, inc=1, device_id=device, device_id_type=MESH)

    for peer in (left, right, far):
        signal((kz, ky, kc, peer))
    for hops in (1, 2, 3):
        signal(above(hops))
    for hop in range(1, PLANE):
        signal(in_plane(lax.rem(kp + hop, PLANE)))
    edge = jnp.logical_or(kz == 0, kz == N_Z - 1)

    def across(p):
        return (N_Z - 1 - kz, p // 2, lax.rem(p, 2), x)

    @pl.when(edge)
    def _():
        for hop in range(1, PLANE):
            signal(across(lax.rem(kp + hop, PLANE)))

    loads = []

    def load(src, dst):
        loads.append(pltpu.make_async_copy(src, dst, load_sem.at[len(loads)]))
        loads[-1].start()
        return loads[-1]

    steps = D // CHUNK
    kv_loads = []
    for k in range(steps):
        rows = pl.ds(k * CHUNK, CHUNK)
        kv_loads.append(
            (
                load(wk_hbm.at[rows], wkv.at[rows, pl.ds(0, 128)]),
                load(wv_hbm.at[rows], wkv.at[rows, pl.ds(128, 128)]),
                load(tok_hbm.at[:, rows], tok.at[:, rows]),
            )
        )
    wq_load = load(wq_hbm, wq)
    wg_load = load(wg_hbm, wg.at[pl.ds(0, 64)])
    wo_load = load(wo_hbm, wall.at[pl.ds(pl.multiple_of(x * WIDTH, WIDTH), WIDTH)])
    with jax.named_scope("barrier_wait"):
        peers_met = PLANE - 1 + N_Z - 1 + N_TP - 1
        pl.semaphore_wait(barrier, peers_met + jnp.where(edge, PLANE - 1, 0))

    def remote(src, dst, send, recv, device):
        return pltpu.make_async_remote_copy(
            src_ref=src,
            dst_ref=dst,
            send_sem=send,
            recv_sem=recv,
            device_id=device,
            device_id_type=MESH,
        )

    def need_copy(p, sender):
        return remote(
            need_ref.at[:, p], asked.at[sender], need_send.at[p], need_recv.at[sender], in_plane(p)
        )

    def peers(fn):
        def step(p, carry):
            @pl.when(p != kp)
            def _():
                fn(p)

            return carry

        lax.fori_loop(0, PLANE, step, 0)

    color = lax.rem(ky + kz, 2)
    mine_row = color * 256 + kc * 128
    other_row = (1 - color) * 256 + kc * 128

    def region(shard, row, count):
        return wall.at[pl.ds(pl.multiple_of(shard * WIDTH + row, 8), count)]

    def w_copy(index, src, dst, device):
        return remote(src, dst, w_send.at[index], w_recv.at[index], device)

    def w_first(side, piece, receiving=False):
        row = mine_row + 32 * piece
        shard = ((left, right)[side]) if receiving else x
        src = region(shard, row, 32)
        dst = src
        if not receiving:
            src = wo_hbm.at[pl.ds(pl.multiple_of(row, 32), 32)]
        return w_copy(4 * side + piece, src, dst, (kz, ky, kc, (right, left)[side]))

    def w_relay(piece, receiving=False):
        side = piece // 2
        part = region(far if receiving else (left, right)[side], mine_row + 32 * piece, 32)
        return w_copy(8 + piece, part, part, (kz, ky, kc, (right, left)[side]))

    directions = (
        (kz, lax.rem(ky + 1, 4), kc, x),
        (kz, lax.rem(ky + 3, 4), kc, x),
        (lax.rem(kz + 1, 4), ky, kc, x),
        (lax.rem(kz + 3, 4), ky, kc, x),
    )
    shards = (left, right, far)

    def slices(o, piece):
        return ((2, 0, 16), (3, 24, 8)) if piece // 2 == o else DIRECTIONS

    def w_second(o, piece, j, first, count, receiving=False, way=None):
        row = (other_row if receiving else mine_row) + 32 * piece + first
        part = region(shards[o], row, count)
        device = directions[j if way is None else way]
        return w_copy(12 + 16 * o + 4 * piece + j, part, part, device)

    def w_swing(o, piece, fn, receiving=False):
        if piece // 2 == o:
            last = kz == N_Z - 1

            @pl.when(jnp.logical_not(last) if receiving else kz != 0)
            def _():
                fn(w_second(o, piece, 1, 16, 8, receiving, 3))

            @pl.when(last if receiving else kz == N_Z - 2)
            def _():
                fn(w_second(o, piece, 0, 16, 8, receiving, 2))

    def w_third(half, o, piece, receiving=False):
        row = (mine_row, other_row)[half] + 32 * piece
        row = row - kc * 128 + (1 - kc) * 128 if receiving else row
        part = region(shards[o], row, 32)
        return w_copy(60 + 12 * half + 4 * o + piece, part, part, (kz, ky, 1 - kc, x))

    def w_spread(o, piece):
        for cut in slices(o, piece):
            w_second(o, piece, *cut).start()
        w_swing(o, piece, lambda copy: copy.start())
        w_third(0, o, piece).start()

    def w_swap(o, pieces):
        for piece in pieces:
            for cut in slices(o, piece):
                w_second(o, piece, *cut, True).wait_recv()
            w_swing(o, piece, lambda copy: copy.wait_recv(), True)
            w_third(1, o, piece).start()

    for piece in range(4):
        w_first(0, piece).start()
        w_first(1, (piece + 2) % 4).start()

    with jax.named_scope("plan"):
        plan = plan_requests(chosen_ref, need_ref)
        need_load = pltpu.make_async_copy(need_ref, need_s, load_sem.at[15])
        need_load.start()
    peers(lambda p: need_copy(p, kp).start())

    def need_far(p, sender):
        return remote(
            need_ref.at[0, p],
            asked_far.at[sender],
            far_send.at[p],
            far_recv.at[sender],
            across(p),
        )

    def everyone(fn):
        def step(p, carry):
            fn(p)
            return carry

        lax.fori_loop(0, PLANE, step, 0)

    @pl.when(kz == N_Z - 1)
    def _():
        everyone(lambda p: need_far(p, kp).start())

    wg[64:] = jnp.zeros((64, D), BF16)

    def clear(d, carry):
        sums[d // PLANE, lax.rem(d, PLANE)] = jnp.zeros(sums.shape[2:], BF16)
        return carry

    lax.fori_loop(me + 1, N_KV, clear, 0)

    with jax.named_scope("kv_proj"):
        for k in range(steps):
            for copy in kv_loads[k]:
                copy.wait()
            ks = slice(k * CHUNK, (k + 1) * CHUNK)
            for rows in HALVES:
                part = nn_dot(tok[rows, ks], wkv[ks])
                acc[rows, :256] = part if k == 0 else acc[rows, :256] + part
    low = lax.broadcasted_iota(jnp.int32, (ROWS, 128), 1) < HD
    keys = acc[:, :128].astype(BF16).astype(F32)
    values = acc[:, 128:256].astype(BF16).astype(F32)
    pairs = (
        jnp.where(low, keys, pltpu.roll(values, HD, 1)),
        jnp.where(low, pltpu.roll(keys, HD, 1), values),
    )
    offsets = pos_ref[...].astype(F32)
    offsets = jnp.concatenate([offsets, offsets], axis=1)
    lane_low = lax.broadcasted_iota(jnp.int32, (CMP, 128), 1) < HD
    row_head = lax.broadcasted_iota(jnp.int32, (8, CMP), 0)
    diagonal = lax.broadcasted_iota(jnp.int32, (CMP, CMP), 0) == lax.broadcasted_iota(
        jnp.int32, (CMP, CMP), 1
    )

    def column(ref, head):
        row = jnp.sum(jnp.where(row_head == head, ref[...].astype(F32), 0.0), axis=0, keepdims=True)
        return jnp.sum(jnp.where(diagonal, row, 0.0), axis=1, keepdims=True)

    with jax.named_scope("summary"):
        tails = []
        for g in range(GROUPS):
            pair = pairs[g]
            blocks = pair.astype(BF16).reshape(BLOCKS, SB, 128)
            unit_0[g] = blocks
            table[4 * N_KV + g * BLOCKS : 4 * N_KV + (g + 1) * BLOCKS] = blocks
            head = x * GROUPS + g
            mixing = jnp.where(lane_low, column(kmix_ref, head), column(vmix_ref, head))
            spans = jnp.sum((pair.reshape(SPANS, CMP, 128) + offsets[None]) * mixing[None], axis=1)
            sums[kz, kp, 16 * g : 16 * g + 16] = spans[:16].astype(BF16)
            tails.append(spans[16:])
        sums[kz, kp, 32:] = jnp.concatenate(tails, axis=0).astype(BF16)

    def lift_copy(hops, receiving=False):
        part = sums.at[kz - hops if receiving else kz, kp]
        return remote(part, part, lift_send.at[hops], lift_recv.at[hops], above(hops))

    def sum_copy(hops, p, sender):
        part = sums.at[kz - hops, sender]
        k = hops * PLANE
        return remote(part, part, sum_send.at[k + p], sum_recv.at[k + sender], in_plane(p))

    def spread(hops, fn):
        def step(p, carry):
            @pl.when(p > kp if hops == 0 else p != kp)
            def _():
                fn(p)

            return carry

        lax.fori_loop(0, PLANE, step, 0)

    def arriving(hops, fn):
        def step(p, carry):
            @pl.when(p < kp if hops == 0 else p != kp)
            def _():
                fn(p)

            return carry

        lax.fori_loop(0, PLANE, step, 0)

    for hops in (1, 2, 3):

        @pl.when(kz + hops < N_Z)
        def _():
            lift_copy(hops).start()

    spread(0, lambda p: sum_copy(0, p, kp).start())

    def unit_copy(hops, g):
        src, dst, k = units[hops - 1].at[g], units[hops].at[g], hops * GROUPS + g
        return remote(src, dst, unit_send.at[k], unit_recv.at[k], above(1))

    sends_unit = {1: kz < 3, 2: jnp.logical_or(kz == 1, kz == 2)}

    @pl.when(sends_unit[1])
    def _():
        for g in range(GROUPS):
            unit_copy(1, g).start()

    with jax.named_scope("gates"):
        wg_load.wait()
        for half, rows in enumerate(HALVES):
            own = pltpu.roll(nt_dot(tok[rows], wg[...]), lax.rem(128 - x * 16, 128), 1)
            part = slice(half * BLOCKS // 2, (half + 1) * BLOCKS // 2)
            gates[part] = jax.nn.sigmoid(own).reshape(BLOCKS // 2, SB, 128)

    with jax.named_scope("plan_blocks"):
        plan_blocks(me, plan, index_ref, bias_ref)
        index_load = pltpu.make_async_copy(index_ref, index_s, load_sem.at[16])
        index_load.start()
    with jax.named_scope("need_wait"):

        def take_need(p):
            need_copy(kp, p).wait_recv()
            pltpu.make_async_copy(asked.at[p], asked_s.at[p], asked_sem.at[p]).start()

        peers(take_need)
        peers(lambda p: pltpu.make_async_copy(asked.at[p], asked_s.at[p], asked_sem.at[p]).wait())
        need_load.wait()
        index_load.wait()

        @pl.when(kz == 0)
        def _():
            def take(p):
                need_far(p, p).wait_recv()
                copy = pltpu.make_async_copy(asked_far.at[p], asked_far_s.at[p], asked_sem.at[p])
                copy.start()
                copy.wait()

            everyone(take)


    def blk_copy(hops, p, sender):
        dst = table.at[pl.ds(((kz - hops) * PLANE + sender) * 4, 4)]
        k = hops * PLANE
        return remote(
            stage.at[hops, p], dst, blk_send.at[k + p], blk_recv.at[k + sender], in_plane(p)
        )

    def unit_pass(g):
        unit_copy(1, g).wait_recv()

        @pl.when(sends_unit[2])
        def _():
            unit_copy(2, g).start()

    def serve(hops):
        @pl.when(kz >= hops)
        def _():
            if hops == 1:
                unit_pass(1)
            if hops == 2:
                for g in range(GROUPS):
                    unit_copy(2, g).wait_recv()

            def one(p):
                for slot in range(4):
                    block = asked_s[p, kz - hops, 0, slot]
                    stage[hops, p, slot] = units[hops][slot // 2, block]
                blk_copy(hops, p, kp).start()

            spread(hops, one)
            if hops:
                for slot in range(4):
                    block = need_s[kz - hops, kp, 0, slot]
                    place = ((kz - hops) * PLANE + kp) * 4 + slot
                    table[place] = units[hops][slot // 2, block]

    with jax.named_scope("sum_pass"):
        for hops in (1, 2, 3):

            @pl.when(kz >= hops)
            def _():
                lift_copy(hops, True).wait_recv()
                spread(hops, lambda p: sum_copy(hops, p, kp).start())

    def far_copy(p, sender):
        return remote(
            stage.at[3, p],
            table.at[pl.ds(sender * 4, 4)],
            blk_send.at[3 * PLANE + p],
            blk_recv.at[3 * PLANE + sender],
            across(p),
        )

    with jax.named_scope("serve_0"):
        serve(0)

        @pl.when(kz == 0)
        def _():
            def one(p):
                for slot in range(4):
                    stage[3, p, slot] = unit_0[slot // 2, asked_far_s[p, 0, slot]]
                far_copy(p, kp).start()

            everyone(one)

    with jax.named_scope("q_proj"):
        wq_load.wait()
        for k in range(steps):
            ks = slice(k * CHUNK, (k + 1) * CHUNK)
            part = nn_dot(tok[:, ks], wq[ks])
            acc[...] = part if k == 0 else acc[...] + part
        for h in range(GROUPS * GROUP):
            tile = acc[:, 128 * (h // 2) : 128 * (h // 2) + 128]
            if h % 2:
                tile = pltpu.roll(tile, HD, 1)
            tile = jnp.where(low, tile, 0.0).astype(BF16) * BF16(HD**-0.5)
            qp[:, h // GROUP, h % GROUP] = tile.reshape(BLOCKS, SB, 128)
    with jax.named_scope("relay"):
        for piece in (0, 2):
            w_first(piece // 2, piece, True).wait_recv()
            w_relay(piece).start()

        @pl.when(kz >= 1)
        def _():
            unit_pass(0)

    with jax.named_scope("sum_wait"):
        for hops in range(N_Z):

            @pl.when(kz >= hops)
            def _():
                arriving(hops, lambda p: sum_copy(hops, kp, p).wait_recv())

    lane = lax.broadcasted_iota(jnp.int32, (SB, N_SPANS), 1)
    tail = lane - N_KV * 16
    span = jnp.where(
        tail < 0,
        (lane // 16) * SPANS + lax.rem(lane, 16),
        (tail // 4) * SPANS + 16 + lax.rem(tail, 4),
    )
    gap = span * CMP + CMP - 1 - lax.broadcasted_iota(jnp.int32, (SB, N_SPANS), 0)
    row_c = lax.rem(lax.broadcasted_iota(jnp.int32, (GROUP * SB, 1), 0), SB)

    def with_ones(pair):
        first = lax.broadcasted_iota(jnp.int32, pair.shape, 1) < HD
        return jnp.where(first, 1.0, pair.astype(F32)).astype(BF16)

    def gate_cols(b, g, branch):
        cols = [
            gates[b][:, 2 * (GROUP * g + r) + branch : 2 * (GROUP * g + r) + branch + 1]
            for r in range(GROUP)
        ]
        return jnp.concatenate(cols, axis=0)

    for g in range(GROUPS):
        tails = [
            sums[s // PLANE, s % PLANE, 32:].astype(F32)[4 * g : 4 * g + 4] for s in range(N_KV)
        ]
        head = sums[:, :, 16 * g : 16 * g + 16].reshape(N_KV * 16, 128)
        tails = jnp.concatenate(tails, axis=0).astype(BF16)
        span_keys[g, : N_KV * 16] = head
        span_keys[g, N_KV * 16 :] = tails
        span_values[g, : N_KV * 16] = with_ones(head)
        span_values[g, N_KV * 16 :] = with_ones(tails)

    def weigh(g, width, biased):
        for c in range(GROUP * SB // STRIP):
            rows = slice(c * STRIP, (c + 1) * STRIP)
            part = biased(score[g, rows, :width], c)
            most = jnp.max(part, axis=1, keepdims=True)
            prob[g, rows, :width] = jnp.exp(part - most).astype(BF16)

    def combine(g, width, table_rows):
        halves = [
            nn_dot(prob[g, h * 128 : (h + 1) * 128, :width], table_rows[...]) for h in range(2)
        ]
        mixed = jnp.concatenate(halves, axis=0)
        return mixed / pltpu.roll(mixed, HD, 1)

    def compressed(b, carry):
        start = me * ROWS + b * SB
        mask[...] = jnp.where(gap <= start, 0.0, LOW)
        for g in range(GROUPS):
            score[g, :, :N_SPANS] = nt_dot(qp[b, g].reshape(GROUP * SB, 128), span_keys[g])

        def biased(part, c):
            first = (c * STRIP) % SB
            return part + mask[first : first + STRIP]

        for g in range(GROUPS):
            weigh(g, N_SPANS, biased)
        for g in range(GROUPS):
            factor = jnp.where(row_c + start >= CMP - 1, gate_cols(b, g, 0), 0.0)
            comp[b, g] = combine(g, N_SPANS, span_values.at[g]) * factor

        @pl.when(b == 0)
        def _():
            with jax.named_scope("serve_1"):
                serve(1)

        @pl.when(b == 1)
        def _():
            with jax.named_scope("relay"):
                for piece in (1, 3):
                    w_first(piece // 2, piece, True).wait_recv()
                    w_relay(piece).start()

        @pl.when(b == 4)
        def _():
            for side in range(2):
                for piece in (2 * side, 2 * side + 1):
                    w_spread(side, piece)

        @pl.when(b == 6)
        def _():
            with jax.named_scope("serve_2"):
                serve(2)

        return carry

    with jax.named_scope("comp"):
        lax.fori_loop(0, BLOCKS, compressed, 0)

    with jax.named_scope("blk_wait"):
        for hops in range(N_Z - 1):

            @pl.when(kz >= hops)
            def _():
                arriving(hops, lambda p: blk_copy(hops, kp, p).wait_recv())

        @pl.when(kz == N_Z - 1)
        def _():
            everyone(lambda p: far_copy(p, p).wait_recv())

    lane_first = lax.broadcasted_iota(jnp.int32, (STRIP, 128), 1)
    row_first = lax.broadcasted_iota(jnp.int32, (STRIP, 128), 0)
    low_half = lax.broadcasted_iota(jnp.int32, (SB, 128), 1) < HD

    def att_copy(target, sender):
        rows = pl.ds(pl.multiple_of(target * OUT_ROWS, 32), OUT_ROWS)
        return remote(
            att.at[rows],
            got.at[sender],
            att_send.at[target],
            att_recv.at[sender],
            (kz, ky, kc, target),
        )

    first_block = lax.rem(5 * (x + 1) // 2, BLOCKS)

    def pass_far(pieces):
        for piece in pieces:
            w_relay(piece, True).wait_recv()
            w_spread(2, piece)

    def chosen_block(i, carry):
        b = lax.rem(first_block + i, BLOCKS)
        for g in range(GROUPS):
            for s in range(N_SEL):
                piece = table[index_s[g, b, s]]
                keys_in[g, s * SB : (s + 1) * SB] = piece
                values_in[g, s * SB : (s + 1) * SB] = with_ones(piece)
            score[g] = nt_dot(qp[b, g].reshape(GROUP * SB, 128), keys_in[g])
        for g in range(GROUPS):

            def biased(part, c):
                part = part + bias_ref[g, b]
                seen = lane_first <= row_first + (c * STRIP) % SB
                seen = jnp.logical_or(lane_first >= SB, seen)
                return jnp.concatenate(
                    [jnp.where(seen, part[:, :128], LOW), part[:, 128:]], axis=1
                )

            weigh(g, N_SEL * SB, biased)
        for g in range(GROUPS):
            both = comp[b, g] + combine(g, N_SEL * SB, values_in.at[g]) * gate_cols(b, g, 1)
            for half in range(2):
                even = both[(2 * half) * SB : (2 * half + 1) * SB]
                odd = both[(2 * half + 1) * SB : (2 * half + 2) * SB]
                tile = jnp.where(low_half, pltpu.roll(even, HD, 1), odd).astype(BF16)
                lanes = slice(256 * g + 128 * half, 256 * g + 128 * half + 128)
                att[pl.ds(pl.multiple_of(b * SB, SB), SB), lanes] = tile
        for hop, last in ((1, 2), (2, 5), (3, 7)):

            @pl.when(i == last)
            def _():
                target = lax.rem(x + hop, N_TP)
                att_copy(target, x).start()

        @pl.when(i == jnp.where(kz == 0, 1, 0))
        def _():
            with jax.named_scope("w1_near"):
                for side in range(2):
                    for piece in (2 - 2 * side, 3 - 2 * side):
                        w_first(side, piece, True).wait_recv()
                        w_spread(side, piece)

        @pl.when(i == BLOCKS - 1)
        def _():
            with jax.named_scope("w2_early"):
                for side in range(2):
                    w_swap(side, (2 * side, 2 * side + 1))

        @pl.when(i == jnp.where(kz == 0, 5, 3))
        def _():
            with jax.named_scope("w1_far"):
                pass_far((0, 2))

        @pl.when(jnp.logical_and(i == 7, kz != 0))
        def _():
            with jax.named_scope("w1_far"):
                pass_far((1, 3))

        return carry

    with jax.named_scope("chosen"):
        lax.fori_loop(0, BLOCKS, chosen_block, 0)

    @pl.when(kz == 0)
    def _():
        with jax.named_scope("w1_far"):
            pass_far((1, 3))


    with jax.named_scope("w2_near"):
        w_swap(0, (2, 3))
        w_swap(1, (0, 1))
    with jax.named_scope("wo_wait"):
        wo_load.wait()
    got[x] = att[pl.ds(pl.multiple_of(x * OUT_ROWS, 32), OUT_ROWS)]
    for order, shard in enumerate((x, left, right, far)):
        if order:
            with jax.named_scope("w3_wait"):
                att_copy(shard, shard).wait_recv()
                for piece in range(4):
                    w_third(0, order - 1, piece, True).wait_recv()
                    w_third(1, order - 1, piece, True).wait_recv()

        def project(n, carry):
            cols = pl.ds(pl.multiple_of(n * CHUNK, CHUNK), CHUNK)
            rows = pl.ds(pl.multiple_of(shard * WIDTH, WIDTH), WIDTH)
            part = nn_dot(got[shard], wall[rows, cols])
            if order:
                part = part + total_ref[:, cols]
            if order < 3:
                total_ref[:, cols] = part
            else:
                out_ref[:, cols] = part.astype(BF16)
            return carry

        with jax.named_scope("outproj"):
            lax.fori_loop(0, D // CHUNK, project, 0)
        if order == 1:
            with jax.named_scope("w2_far"):
                w_swap(2, range(4))

    with jax.named_scope("drain"):
        peers(lambda p: need_copy(p, kp).wait_send())

        @pl.when(kz == N_Z - 1)
        def _():
            everyone(lambda p: need_far(p, kp).wait_send())

        @pl.when(kz == 0)
        def _():
            everyone(lambda p: far_copy(p, kp).wait_send())

        for piece in range(4):
            w_first(0, piece).wait_send()
            w_first(1, piece).wait_send()
            w_relay(piece).wait_send()
            for o in range(3):
                for cut in slices(o, piece):
                    w_second(o, piece, *cut).wait_send()
                w_swing(o, piece, lambda copy: copy.wait_send())
                w_third(0, o, piece).wait_send()
                w_third(1, o, piece).wait_send()
        for hop in (1, 2, 3):
            att_copy(lax.rem(x + hop, N_TP), x).wait_send()
        for hops in (1, 2, 3):

            @pl.when(kz + hops < N_Z)
            def _():
                lift_copy(hops).wait_send()

        for hops in (1, 2):

            @pl.when(sends_unit[hops])
            def _():
                for g in range(GROUPS):
                    unit_copy(hops, g).wait_send()

        for hops in range(N_Z):

            @pl.when(kz >= hops)
            def _():
                def done(p):
                    sum_copy(hops, p, kp).wait_send()
                    if hops < 3:
                        blk_copy(hops, p, kp).wait_send()

                spread(hops, done)


def local(
    tokens,
    query_weight,
    key_weight,
    value_weight,
    gate_weight,
    summary_pos,
    key_mixing,
    value_mixing,
    out_weight,
    chosen,
):
    any_space = pl.BlockSpec(memory_space=pltpu.HBM)
    vmem = pl.BlockSpec(memory_space=pltpu.VMEM)
    dma = pltpu.SemaphoreType.DMA
    unit = pltpu.VMEM((GROUPS, BLOCKS, SB, 128), BF16)
    requests = (N_Z, PLANE, 1, 128)
    return pl.pallas_call(
        body,
        out_shape=pltpu.VMEM((OUT_ROWS, D), BF16),
        in_specs=[any_space] * 5 + [vmem] * 3 + [any_space, vmem],
        out_specs=vmem,
        scratch_shapes=[
            pltpu.VMEM((ROWS, D), BF16),
            pltpu.VMEM((D, WIDTH), BF16),
            pltpu.VMEM((D, 256), BF16),
            pltpu.VMEM((128, D), BF16),
            pltpu.VMEM((ROWS, WIDTH), F32),
            pltpu.VMEM((BLOCKS, SB, 128), F32),
            pltpu.VMEM((BLOCKS, GROUPS, GROUP, SB, 128), BF16),
            pltpu.VMEM((N_Z, PLANE, 40, 128), BF16),
            pltpu.VMEM((PLANE, N_Z, 1, 128), jnp.int32),
            pltpu.SMEM((PLANE, N_Z, 1, 128), jnp.int32),
            pltpu.VMEM((PLANE, 1, 128), jnp.int32),
            pltpu.SMEM((PLANE, 1, 128), jnp.int32),
            pltpu.VMEM((4 * N_KV + GROUPS * BLOCKS, SB, 128), BF16),
            pltpu.VMEM((N_Z, PLANE, 4, SB, 128), BF16),
            unit,
            unit,
            unit,
            pltpu.VMEM((BLOCKS, GROUPS, GROUP * SB, 128), F32),
            pltpu.VMEM((GROUPS, GROUP * SB, N_SEL * SB), F32),
            pltpu.VMEM((GROUPS, GROUP * SB, N_SEL * SB), BF16),
            pltpu.VMEM((GROUPS, N_SEL * SB, 128), BF16),
            pltpu.VMEM((GROUPS, N_SEL * SB, 128), BF16),
            pltpu.VMEM((GROUPS, N_SPANS, 128), BF16),
            pltpu.VMEM((GROUPS, N_SPANS, 128), BF16),
            pltpu.VMEM((SB, N_SPANS), F32),
            pltpu.VMEM(requests, jnp.int32),
            pltpu.SMEM(requests, jnp.int32),
            pltpu.VMEM((GROUPS, 16, 128), jnp.int32),
            pltpu.SMEM((GROUPS, 16, 128), jnp.int32),
            pltpu.VMEM((GROUPS, BLOCKS, 1, N_SEL * SB), F32),
            pltpu.VMEM((N_TP * WIDTH, D), BF16),
            pltpu.VMEM((ROWS, WIDTH), BF16),
            pltpu.VMEM((N_TP, OUT_ROWS, WIDTH), BF16),
            pltpu.VMEM((OUT_ROWS, D), F32),
            dma((17,)),
            dma((PLANE,)),
            dma((84,)),
            dma((84,)),
            dma((N_TP,)),
            dma((N_TP,)),
            dma((PLANE,)),
            dma((PLANE,)),
            dma((PLANE,)),
            dma((PLANE,)),
            dma((N_Z,)),
            dma((N_Z,)),
            dma((N_Z * GROUPS,)),
            dma((N_Z * GROUPS,)),
            dma((N_KV,)),
            dma((N_KV,)),
            dma((N_KV,)),
            dma((N_KV,)),
        ],
        compiler_params=pltpu.CompilerParams(
            collective_id=0, has_side_effects=True, vmem_limit_bytes=VMEM_MIB * 1024 * 1024
        ),
    )(
        tokens,
        query_weight,
        key_weight,
        value_weight,
        gate_weight.T,
        summary_pos,
        key_mixing.T,
        value_mixing.T,
        out_weight,
        chosen,
    )


def solution(mesh):
    torus = Mesh(mesh.devices.reshape(4, 4, 2, mesh.shape["tp"]), ("kv_0", "kv_1", "kv_2", "tp"))
    in_specs = (
        P(KV, None),
        P(None, "tp"),
        P(None, "tp"),
        P(None, "tp"),
        P(),
        P(),
        P(),
        P(),
        P("tp", None),
        P(KV, "tp", None),
    )
    out_specs = P(KV_TP, None)
    return jax.shard_map(local, mesh=torus, in_specs=in_specs, out_specs=out_specs, check_vma=False)
```
